512 devices in a mesh: sp: 16 (over z), dp: 32 (over y, x, core).
Axes of the slice: x: 4, y: 4, z: 16, core: 2. Of those that a mesh axis runs over, the one named last changes fastest.
Arguments:
- inputs: bfloat16 [32, 2048, 2048], P('dp', 'sp'), may hold values from -0.75 to 0.75
- queries: bfloat16 [32, 2048, 1024], P('dp', 'sp'), may hold values from -18 to 18
- keys: bfloat16 [32, 2048, 256], P('dp', 'sp'), may hold values from -18 to 18
- values: bfloat16 [32, 2048, 256], P('dp', 'sp'), may hold values from -6 to 6
- out_grad: bfloat16 [32, 2048, 1024], P('dp', 'sp'), may hold values from -144 to 144
- query_gain: float32 [64], replicated, may hold values from 0.4 to 6.5
- key_gain: float32 [64], replicated, may hold values from 0.4 to 6.5
- key_matrix: bfloat16 [2048, 256], P('dp'), may hold values from -0.125 to 0.125
- value_matrix: bfloat16 [2048, 256], P('dp'), may hold values from -0.125 to 0.125
Outputs:
- input_grad: bfloat16 [32, 2048, 2048], P('dp', 'sp')
- query_grad: bfloat16 [32, 2048, 1024], P('dp', 'sp')
- key_weight_grad: float32 [2048, 256], P('dp')
- value_weight_grad: float32 [2048, 256], P('dp')
The draws below stay inside these ranges and needn't reach their ends.
All inputs are finite; a program needn't handle non-finite values.
Results may differ from the reference program's by a relative error of at most 0.024.
The reference program's roundings to bfloat16 on the way count: a program that leaves them out, or rounds other values in their place, can miss the bound.
Values may be sent and summed in bfloat16 or wider, within the bound.
A program may use at most 64 MiB of HBM per device.

```python
import jax
import jax.numpy as jnp
from jax import lax

MODEL_WIDTH = 2048
QUERY_HEADS = 16
KEY_VALUE_HEADS = 4
HEAD_CHANNELS = 64
GRID = 64
SEQUENCE_LENGTH = 2048
SEQUENCE_COUNT = 32
HPART = 1


def gain_draw(seed_key):
    return jnp.clip(1.0 + 0.18 * jax.random.normal(seed_key, (HEAD_CHANNELS,), jnp.float32), 0.4, 1.6)


def draw_query_gain(key, part):
    return gain_draw(jax.random.fold_in(key, 11))


def draw_key_gain(key, part):
    return gain_draw(jax.random.fold_in(key, 23))


def level_of(stream_key, extent, cuts, low, largest):
    def one(dim, parts):
        steps = jax.random.uniform(jax.random.fold_in(jax.random.fold_in(stream_key, 6), dim), (parts,), jnp.float32, low / len(cuts), largest / len(cuts))
        return jnp.repeat(jnp.exp(steps), extent[dim] // parts).reshape((-1,) + (1,) * (len(extent) - dim - 1))

    level = one(*cuts[0])
    for cut in cuts[1:]:
        level = level * one(*cut)
    return level


def bell_draw(rng, shape, deviation, limit, shards=(), kind=jnp.bfloat16):
    entries = jax.random.normal(rng, shape, jnp.float32) * deviation
    if len(shards) > 0:
        entries = level_of(rng, shape, shards, -0.22, 0.18) * entries
    return jnp.clip(entries, min=-limit, max=limit).astype(kind)


def setup_inputs(seed: int = 0) -> dict:
    arg_keys = jax.random.split(jax.random.key(seed), 10)
    return {
        "inputs": bell_draw(arg_keys[0], (SEQUENCE_COUNT, SEQUENCE_LENGTH, MODEL_WIDTH), 0.125, 0.75, ((0, 32), (1, 16))),
        "queries": bell_draw(arg_keys[1], (SEQUENCE_COUNT, SEQUENCE_LENGTH, QUERY_HEADS * HEAD_CHANNELS), 3.0, 18.0, ((0, 32), (1, 16))),
        "keys": bell_draw(arg_keys[2], (SEQUENCE_COUNT, SEQUENCE_LENGTH, KEY_VALUE_HEADS * HEAD_CHANNELS), 3.0, 18.0, ((0, 32), (1, 16))),
        "values": bell_draw(arg_keys[3], (SEQUENCE_COUNT, SEQUENCE_LENGTH, KEY_VALUE_HEADS * HEAD_CHANNELS), 1.0, 6.0, ((0, 32), (1, 16))),
        "out_grad": bell_draw(arg_keys[4], (SEQUENCE_COUNT, SEQUENCE_LENGTH, QUERY_HEADS * HEAD_CHANNELS), 24.0, 144.0, ((0, 32), (1, 16))),
        "query_gain": draw_query_gain(jax.random.fold_in(arg_keys[9], 71), 0),
        "key_gain": draw_key_gain(jax.random.fold_in(arg_keys[9], 71), 0),
        "key_matrix": bell_draw(arg_keys[7], (MODEL_WIDTH, KEY_VALUE_HEADS * HEAD_CHANNELS), MODEL_WIDTH ** -0.5, 0.125, ((0, 32),)),
        "value_matrix": bell_draw(arg_keys[8], (MODEL_WIDTH, KEY_VALUE_HEADS * HEAD_CHANNELS), MODEL_WIDTH ** -0.5, 0.125, ((0, 32),)),
    }


rope_base = 10000.0
norm_eps = 0.5
score_scale = 0.125

def product(pattern, first_op, second_op):
    return jnp.einsum(pattern, first_op.astype(jnp.float32), second_op.astype(jnp.float32))

def rotary_tables(token_length):
    position = jnp.arange(token_length, dtype=jnp.int32)
    grid_row = (position // GRID).astype(jnp.float32)
    grid_col = (position % GRID).astype(jnp.float32)
    half_pairs = HEAD_CHANNELS // 4
    inv_freq = rope_base ** (-jnp.arange(half_pairs, dtype=jnp.float32) / half_pairs)
    angles = jnp.concatenate([grid_row[:, None] * inv_freq, grid_col[:, None] * inv_freq], axis=1)
    return (jnp.cos(angles), jnp.sin(angles))

def rotate(vector, cos_tab, sin_tab):
    even_part = vector[..., 0::2]
    odd_part = vector[..., 1::2]
    turned = jnp.stack([even_part * cos_tab - odd_part * sin_tab, even_part * sin_tab + odd_part * cos_tab], axis=-1)
    return turned.reshape(vector.shape)

def rotate_back(cotangent, cos_tab, sin_tab):
    even_part = cotangent[..., 0::2]
    odd_part = cotangent[..., 1::2]
    turned = jnp.stack([even_part * cos_tab + odd_part * sin_tab, odd_part * cos_tab - even_part * sin_tab], axis=-1)
    return turned.reshape(cotangent.shape)

def inverse_rms(vector):
    return lax.rsqrt(lax.optimization_barrier(jnp.mean(vector * vector, axis=-1, keepdims=True)) + norm_eps)

def norm_back(vector, inv_scale, cotangent, gain_vec):
    weighted = cotangent * gain_vec
    inner_mean = lax.optimization_barrier(jnp.mean(weighted * vector, axis=-1, keepdims=True))
    return inv_scale * (weighted - vector * inv_scale * inv_scale * inner_mean)

def head_grads(query_in, key_input, value_input, grad_in, query_gain, key_gain, cos_tab, sin_tab, block_rows):
    token_length, groups, per_group, head_dim = query_in.shape
    cos_four = cos_tab[:, None, None, :]
    sin_four = sin_tab[:, None, None, :]
    cos_three = cos_tab[:, None, :]
    sin_three = sin_tab[:, None, :]
    query_f = query_in.astype(jnp.float32)
    query_inv = inverse_rms(query_f)
    query_rot = rotate(query_f * query_inv * query_gain, cos_four, sin_four).astype(jnp.bfloat16)
    key_f = key_input.astype(jnp.float32)
    key_inv = inverse_rms(key_f)
    key_rot = rotate(key_f * key_inv * key_gain, cos_three, sin_three).astype(jnp.bfloat16)
    num_blocks = token_length // block_rows
    query_blocks = query_rot.reshape(num_blocks, block_rows, groups, per_group, head_dim)
    grad_blocks = grad_in.reshape(num_blocks, block_rows, groups, per_group, head_dim)

    def attend_block(carried, pieces):
        key_acc, value_acc = carried
        query_piece, grad_piece = pieces
        scores = product('qgrd,cgd->grqc', query_piece, key_rot) * score_scale
        row_max = lax.optimization_barrier(jnp.max(scores, axis=-1, keepdims=True))
        shifted = jnp.exp(scores - row_max)
        attn_prob = shifted / lax.optimization_barrier(jnp.sum(shifted, axis=-1, keepdims=True))
        prob_low = attn_prob.astype(jnp.bfloat16)
        prob_grad = product('qgrd,cgd->grqc', grad_piece, value_input)
        row_dot = lax.optimization_barrier(jnp.sum(attn_prob * prob_grad, axis=-1, keepdims=True))
        score_grad = (attn_prob * (prob_grad - row_dot) * score_scale).astype(jnp.bfloat16)
        dq_piece = product('grqc,cgd->qgrd', score_grad, key_rot)
        key_acc = key_acc + product('grqc,qgrd->cgd', score_grad, query_piece)
        value_acc = value_acc + product('grqc,qgrd->cgd', prob_low, grad_piece)
        return ((key_acc, value_acc), dq_piece)
    empty_acc = jnp.zeros((token_length, groups, head_dim), jnp.float32)
    (key_rot_grad, value_acc), query_rot_grad = lax.scan(attend_block, (empty_acc, empty_acc), (query_blocks, grad_blocks))
    query_rot_grad = query_rot_grad.reshape(token_length, groups, per_group, head_dim)
    query_grad = norm_back(query_f, query_inv, rotate_back(query_rot_grad, cos_four, sin_four), query_gain).astype(jnp.bfloat16)
    key_portion = norm_back(key_f, key_inv, rotate_back(key_rot_grad, cos_three, sin_three), key_gain).astype(jnp.bfloat16)
    return (query_grad, key_portion, value_acc.astype(jnp.bfloat16))

def reference(inputs, queries, keys, values, out_grad, query_gain, key_gain, key_matrix, value_matrix):
    token_length = queries.shape[1]
    portion_count = QUERY_HEADS // HPART
    group_copies = portion_count // KEY_VALUE_HEADS
    cos_tab, sin_tab = rotary_tables(token_length)
    block_rows = min(512, token_length)

    def sequence_grads(pack):
        query_in, key_input, value_input, grad_in = pack
        key_positions = jnp.repeat(key_input.reshape(token_length, KEY_VALUE_HEADS, HEAD_CHANNELS), group_copies, axis=1)
        value_positions = jnp.repeat(value_input.reshape(token_length, KEY_VALUE_HEADS, HEAD_CHANNELS), group_copies, axis=1)
        query_part, key_portion, value_portion = head_grads(query_in.reshape(token_length, portion_count, HPART, HEAD_CHANNELS), key_positions, value_positions, grad_in.reshape(token_length, portion_count, HPART, HEAD_CHANNELS), query_gain, key_gain, cos_tab, sin_tab, block_rows)
        key_gradient = key_portion.reshape(token_length, KEY_VALUE_HEADS, group_copies, HEAD_CHANNELS).astype(jnp.float32).sum(axis=2).astype(jnp.bfloat16)
        value_gradient = value_portion.reshape(token_length, KEY_VALUE_HEADS, group_copies, HEAD_CHANNELS).astype(jnp.float32).sum(axis=2).astype(jnp.bfloat16)
        joined_output = jnp.concatenate([key_gradient.reshape(token_length, KEY_VALUE_HEADS * HEAD_CHANNELS), value_gradient.reshape(token_length, KEY_VALUE_HEADS * HEAD_CHANNELS)], axis=1)
        return (query_part.reshape(token_length, QUERY_HEADS * HEAD_CHANNELS), joined_output)
    query_grad, projection_gradient = lax.map(sequence_grads, (queries, keys, values, out_grad))
    joined_weight = jnp.concatenate([key_matrix, value_matrix], axis=1)
    flattened_gradient = projection_gradient.reshape(-1, 2 * KEY_VALUE_HEADS * HEAD_CHANNELS)
    input_grad = jnp.dot(flattened_gradient, joined_weight.T, preferred_element_type=jnp.float32).astype(jnp.bfloat16)
    input_grad = input_grad.reshape(inputs.shape)
    weight_grad = jnp.dot(inputs.reshape(-1, inputs.shape[2]).T, flattened_gradient, preferred_element_type=jnp.float32)
    key_value_width = KEY_VALUE_HEADS * HEAD_CHANNELS
    return (input_grad, query_grad, weight_grad[:, :key_value_width], weight_grad[:, key_value_width:])
```

```python
import functools

import jax
import jax.numpy as jnp
from jax import lax
from jax.experimental import pallas as pl
from jax.experimental.pallas import tpu as pltpu
from jax.sharding import PartitionSpec as P

GROUPS = 4
PER = 4
DIM = 64
HALF = 32
GRID = 64
ROPE_BASE = 10000.0
EPS = 0.5
SCALE = 0.125
KVW = GROUPS * DIM
F32 = jnp.float32
BF16 = jnp.bfloat16

NN = (((1,), (0,)), ((), ()))
NT = (((1,), (1,)), ((), ()))
TN = (((0,), (0,)), ((), ()))


def dot(a, b, dims=NN):
    return lax.dot_general(a, b, dims, preferred_element_type=F32)


def split_pairs(transposed=False):
    r = lax.broadcasted_iota(jnp.int32, (KVW, KVW), 1 if transposed else 0)
    c = lax.broadcasted_iota(jnp.int32, (KVW, KVW), 0 if transposed else 1)
    i = r % DIM
    src = r - i + jnp.where(i < HALF, 2 * i, 2 * i - (DIM - 1))
    return (c == src).astype(F32).astype(BF16)


def eye(n):
    r = lax.broadcasted_iota(jnp.int32, (n, n), 0)
    c = lax.broadcasted_iota(jnp.int32, (n, n), 1)
    return (r == c).astype(F32).astype(BF16)


def inv_rms(a, b):
    ms = (jnp.sum(a * a, axis=0, keepdims=True) + jnp.sum(b * b, axis=0, keepdims=True)) * (1.0 / DIM)
    return lax.rsqrt(ms + EPS)


def rope_fwd(x, cos, sin, gain):
    a, b = x[:HALF], x[HALF:]
    r = inv_rms(a, b)
    a = a * r * gain[:HALF]
    b = b * r * gain[HALF:]
    return jnp.concatenate([a * cos - b * sin, a * sin + b * cos], axis=0)


def rope_bwd(g, x, cos, sin, gain):
    a, b = g[:HALF], g[HALF:]
    ua = (a * cos + b * sin) * gain[:HALF]
    ub = (b * cos - a * sin) * gain[HALF:]
    qa, qb = x[:HALF], x[HALF:]
    r = inv_rms(qa, qb)
    inner = (jnp.sum(ua * qa, axis=0, keepdims=True) + jnp.sum(ub * qb, axis=0, keepdims=True)) * (1.0 / DIM)
    f = r * r * inner
    return jnp.concatenate([r * (ua - qa * f), r * (ub - qb * f)], axis=0)


def prep_kernel(k_ref, v_ref, cs_ref, gain_ref, kv_ref):
    t = k_ref.shape[0]
    cos, sin = cs_ref[:HALF], cs_ref[HALF:]
    xt = dot(split_pairs(), k_ref[...], NT)
    gain = gain_ref[DIM:]
    rot = jnp.concatenate(
        [rope_fwd(xt[DIM * h : DIM * (h + 1)], cos, sin, gain) for h in range(GROUPS)], axis=0
    ).astype(BF16)
    kv_ref[:t] = dot(eye(t), rot, NT).astype(BF16)
    kv_ref[t:] = v_ref[...]


def attn_kernel(
    q_ref, do_ref, kv_ref, cs_ref, gain_ref, qg_ref, dkv_ref,
    qbd, qbdt, obd, obdt, e_ref, dp_ref, mj, mrun, lsum, dsum, qt, dqt,
):
    t = q_ref.shape[0]
    n = kv_ref.shape[0]
    w = PER * t
    cos, sin = cs_ref[:HALF], cs_ref[HALF:]
    gain = gain_ref[:DIM]
    perm = split_pairs()
    ident = eye(t)
    ident_w = eye(KVW)
    qbd[...] = jnp.zeros_like(qbd)
    obd[...] = jnp.zeros_like(obd)
    for g in range(GROUPS):
        xt = dot(perm, q_ref[:, KVW * g : KVW * (g + 1)], NT)
        qt[g] = xt
        ot = dot(ident_w, do_ref[:, KVW * g : KVW * (g + 1)], NT).astype(BF16)
        for h in range(PER):
            rows = slice(DIM * h, DIM * (h + 1))
            rot = rope_fwd(xt[rows], cos, sin, gain).astype(BF16) * jnp.asarray(SCALE, BF16)
            cols = slice(w * g + t * h, w * g + t * (h + 1))
            qbd[DIM * g : DIM * (g + 1), cols] = rot
            obd[DIM * g : DIM * (g + 1), cols] = ot[rows]
    for i in range(GROUPS * PER):
        cols = slice(t * i, t * (i + 1))
        qbdt[cols, :] = dot(ident, qbd[:, cols], NT).astype(BF16)
        obdt[cols, :] = dot(ident, obd[:, cols], NT).astype(BF16)

    mrun[...] = jnp.full_like(mrun, -jnp.inf)
    lsum[...] = jnp.zeros_like(lsum)
    dsum[...] = jnp.zeros_like(dsum)
    dqt[...] = jnp.zeros_like(dqt)

    def gather_block(j, _):
        kb = kv_ref[j, :t]
        vb = kv_ref[j, t:]
        for g in range(GROUPS):
            cols = slice(w * g, w * (g + 1))
            s = dot(kb, qbd[:, cols])
            dp = dot(vb, obd[:, cols])
            m_old = mrun[:, cols]
            m_new = jnp.maximum(m_old, jnp.max(s, axis=0, keepdims=True))
            e = jnp.exp(s - m_new)
            a = jnp.exp(m_old - m_new)
            mrun[:, cols] = m_new
            mj[j, :, cols] = m_new
            lsum[:, cols] = lsum[:, cols] * a + jnp.sum(e, axis=0, keepdims=True)
            dsum[:, cols] = dsum[:, cols] * a + jnp.sum(e * dp, axis=0, keepdims=True)
            e_ref[j, :, cols] = e
            dp_ref[j, :, cols] = dp
        return 0

    lax.fori_loop(0, n, gather_block, 0)
    lsum[...] = 1.0 / lsum[...]
    dsum[...] = dsum[...] * lsum[...]

    def back_block(j, _):
        kt = dot(ident_w, kv_ref[j, :t], NT).astype(BF16)
        dk = jnp.zeros((t, KVW), F32)
        dv = jnp.zeros((t, KVW), F32)
        for g in range(GROUPS):
            cols = slice(w * g, w * (g + 1))
            c = jnp.exp(mj[j, :, cols] - mrun[:, cols]) * lsum[:, cols]
            p = e_ref[j, :, cols] * c
            ds = (p * (dp_ref[j, :, cols] - dsum[:, cols])).astype(BF16)
            dv += dot(p.astype(BF16), obdt[cols, :])
            dk += dot(ds, qbdt[cols, :])
            dqt[DIM * g : DIM * (g + 1)] += dot(kt[DIM * g : DIM * (g + 1)], ds)
        dkv_ref[j, :t] = dk.astype(BF16)
        dkv_ref[j, t:] = dv.astype(BF16)
        return 0

    lax.fori_loop(0, n, back_block, 0)

    perm_t = split_pairs(True)
    for g in range(GROUPS):
        y = jnp.concatenate(
            [
                rope_bwd(
                    dqt[DIM * g : DIM * (g + 1), t * h : t * (h + 1)] * SCALE,
                    qt[g, DIM * h : DIM * (h + 1)], cos, sin, gain,
                )
                for h in range(PER)
            ],
            axis=0,
        ).astype(BF16)
        y = dot(perm_t, y).astype(BF16)
        qg_ref[:, KVW * g : KVW * (g + 1)] = dot(ident, y, NT).astype(BF16)


def finish_kernel(dkv_ref, k_ref, cs_ref, gain_ref, in_ref, w_ref, ig_ref, wp_ref):
    t = k_ref.shape[0]
    cos, sin = cs_ref[:HALF], cs_ref[HALF:]
    gain = gain_ref[DIM:]
    xt = dot(split_pairs(), k_ref[...], NT)
    gt = dot(eye(KVW), dkv_ref[:t], NT)
    y = jnp.concatenate(
        [
            rope_bwd(gt[DIM * h : DIM * (h + 1)], xt[DIM * h : DIM * (h + 1)], cos, sin, gain)
            for h in range(GROUPS)
        ],
        axis=0,
    ).astype(BF16)
    y = dot(split_pairs(True), y).astype(BF16)
    pg = jnp.concatenate([dot(eye(t), y, NT).astype(BF16), dkv_ref[t:]], axis=1)
    ig_ref[...] = dot(pg, w_ref[...], NT).astype(BF16)
    wp_ref[...] = dot(in_ref[...], pg, TN).astype(BF16)


def tables(t):
    pos = lax.axis_index("sp") * t + jnp.arange(t, dtype=jnp.int32)
    row = (pos // GRID).astype(F32)
    col = (pos % GRID).astype(F32)
    m = DIM // 4
    inv = ROPE_BASE ** (-jnp.arange(m, dtype=F32) / m)
    ang = jnp.concatenate([inv[:, None] * row, inv[:, None] * col], axis=0)
    return jnp.concatenate([jnp.cos(ang), jnp.sin(ang)], axis=0)


def split_gain(g, t):
    g = jnp.concatenate([g[0::2], g[1::2]])
    return jnp.broadcast_to(g[:, None], (DIM, t))


def params():
    return pltpu.CompilerParams(vmem_limit_bytes=60 * 1024 * 1024)


def on_device(inputs, queries, keys, values, out_grad, query_gain, key_gain, key_matrix, value_matrix):
    n = lax.axis_size("sp")
    t = inputs.shape[1]
    s = n * t
    q_all = GROUPS * PER * t
    cs = tables(t)
    gains = jnp.concatenate([split_gain(query_gain, t), split_gain(key_gain, t)], axis=0)
    kv = pl.pallas_call(
        prep_kernel, out_shape=jax.ShapeDtypeStruct((2 * t, KVW), BF16), compiler_params=params()
    )(keys[0], values[0], cs, gains)
    kv_all = lax.all_gather(kv, "sp", axis=0, tiled=False)
    w_all = lax.all_gather(jnp.concatenate([key_matrix, value_matrix], axis=1), "dp", axis=0, tiled=True)
    query_grad, dkv = pl.pallas_call(
        attn_kernel,
        out_shape=(
            jax.ShapeDtypeStruct((t, GROUPS * PER * DIM), BF16),
            jax.ShapeDtypeStruct((n, 2 * t, KVW), BF16),
        ),
        scratch_shapes=[
            pltpu.VMEM((KVW, q_all), BF16),
            pltpu.VMEM((q_all, KVW), BF16),
            pltpu.VMEM((KVW, q_all), BF16),
            pltpu.VMEM((q_all, KVW), BF16),
            pltpu.VMEM((n, t, q_all), F32),
            pltpu.VMEM((n, t, q_all), F32),
            pltpu.VMEM((n, 1, q_all), F32),
            pltpu.VMEM((1, q_all), F32),
            pltpu.VMEM((1, q_all), F32),
            pltpu.VMEM((1, q_all), F32),
            pltpu.VMEM((GROUPS, KVW, t), F32),
            pltpu.VMEM((KVW, PER * t), F32),
        ],
        compiler_params=params(),
    )(queries[0], out_grad[0], kv_all, cs, gains)
    mine = lax.psum_scatter(dkv, "sp", scatter_dimension=0, tiled=False)
    input_grad, w_part = pl.pallas_call(
        finish_kernel,
        out_shape=(
            jax.ShapeDtypeStruct((t, inputs.shape[2]), BF16),
            jax.ShapeDtypeStruct((inputs.shape[2], 2 * KVW), BF16),
        ),
        compiler_params=params(),
    )(mine, keys[0], cs, gains, inputs[0], w_all)
    w_mine = lax.psum_scatter(w_part, "dp", scatter_dimension=0, tiled=True)
    w_grad = lax.psum(w_mine.astype(F32), "sp")
    return input_grad[None], query_grad[None], w_grad[:, :KVW], w_grad[:, KVW:]


def solution(mesh):
    row = P("dp", "sp", None)
    return jax.shard_map(
        on_device,
        mesh=mesh,
        in_specs=(row, row, row, row, row, P(), P(), P("dp", None), P("dp", None)),
        out_specs=(row, row, P("dp", None), P("dp", None)),
        check_vma=False,
    )
```

```python
import functools

import jax
import jax.numpy as jnp
import numpy as np
from jax import lax
from jax.experimental import pallas as pl
from jax.experimental.pallas import tpu as pltpu
from jax.sharding import PartitionSpec as P

GROUPS = 4
PER = 4
DIM = 64
HALF = 32
GRID = 64
ROPE_BASE = 10000.0
EPS = 0.5
SCALE = 0.125
KVW = GROUPS * DIM
HALFW = 2 * DIM
CHUNKS = 4
F32 = jnp.float32
BF16 = jnp.bfloat16
MESH = pl.DeviceIdType.MESH

NN = (((1,), (0,)), ((), ()))
NT = (((1,), (1,)), ((), ()))


def dot(a, b, dims=NN):
    return lax.dot_general(a, b, dims, preferred_element_type=F32)


def split_source(shape, axis):
    r = lax.broadcasted_iota(jnp.int32, shape, axis)
    i = r % DIM
    return r - i + jnp.where(i < HALF, 2 * i, 2 * i - (DIM - 1))


def split_pairs(transposed=False):
    axis = 1 if transposed else 0
    c = lax.broadcasted_iota(jnp.int32, (KVW, KVW), 1 - axis)
    return (c == split_source((KVW, KVW), axis)).astype(F32).astype(BF16)


def split_gain(gain):
    c = lax.broadcasted_iota(jnp.int32, (DIM, DIM), 1)
    pick = c == split_source((DIM, DIM), 0)
    return jnp.sum(jnp.where(pick, gain, 0.0), axis=1, keepdims=True)


def eye(n):
    r = lax.broadcasted_iota(jnp.int32, (n, n), 0)
    c = lax.broadcasted_iota(jnp.int32, (n, n), 1)
    return (r == c).astype(F32).astype(BF16)


def inv_rms(a, b):
    ms = (jnp.sum(a * a, axis=0, keepdims=True) + jnp.sum(b * b, axis=0, keepdims=True)) * (1.0 / DIM)
    return lax.rsqrt(ms + EPS)


def rope_fwd(x, cos, sin, gain):
    a, b = x[:HALF], x[HALF:]
    r = inv_rms(a, b)
    a = a * r * gain[:HALF]
    b = b * r * gain[HALF:]
    return jnp.concatenate([a * cos - b * sin, a * sin + b * cos], axis=0)


def rope_bwd(g, x, cos, sin, gain):
    a, b = g[:HALF], g[HALF:]
    ua = (a * cos + b * sin) * gain[:HALF]
    ub = (b * cos - a * sin) * gain[HALF:]
    qa, qb = x[:HALF], x[HALF:]
    r = inv_rms(qa, qb)
    inner = (jnp.sum(ua * qa, axis=0, keepdims=True) + jnp.sum(ub * qb, axis=0, keepdims=True)) * (1.0 / DIM)
    f = r * r * inner
    return jnp.concatenate([r * (ua - qa * f), r * (ub - qb * f)], axis=0)


def kernel(
    n, nd,
    x_ref, q_ref, k_ref, v_ref, do_ref, qgain_ref, kgain_ref, km_ref, vm_ref, tab_ref,
    ig_ref, qg_ref, kw_ref, vw_ref,
    cs, kvb, w_all, qbd, qbdt, obd, obdt, e_ref, dp_ref, mj, mrun, lsum, dsum, qt, kt, xt, dqt, acc,
    sbuf, rbuf, wp, pbuf, asend, arecv, zsend, zrecv, zall,
    tab_sem, g_send, g_recv, w_send, w_recv, r_send, r_recv, p_send, p_recv, a_send, a_recv,
    z_send, z_recv, y_send, y_recv,
):
    t = q_ref.shape[0]
    w = PER * t
    h = n // 2
    crow = 2 * t // CHUNKS
    wrow = km_ref.shape[0]
    chips = nd // 2
    me = lax.axis_index("sp")
    dme = lax.axis_index("dp")
    core = dme % 2
    chip = dme // 2
    right = (me + 1) % n
    left = (me + n - 1) % n

    table = pltpu.make_async_copy(tab_ref.at[me], cs, tab_sem)
    table.start()
    barrier = pltpu.get_barrier_semaphore()

    def greet_sp(k, _):
        pl.semaphore_signal(barrier, inc=1, device_id={"sp": (me + k) % n}, device_id_type=MESH)
        return 0

    def greet_dp(k, _):
        pl.semaphore_signal(barrier, inc=1, device_id={"dp": (dme + k) % nd}, device_id_type=MESH)
        return 0

    lax.fori_loop(1, n, greet_sp, 0)
    lax.fori_loop(1, nd, greet_dp, 0)

    perm = split_pairs()
    ident = eye(t)
    ident_w = eye(KVW)
    qgain = split_gain(qgain_ref[...])
    kgain = split_gain(kgain_ref[...])
    kt[...] = dot(perm, k_ref[...], NT)
    w_rows = pl.ds(dme * wrow, wrow)
    w_all[w_rows, :KVW] = km_ref[...]
    w_all[w_rows, KVW:] = vm_ref[...]
    table.wait()
    cos, sin = cs[:HALF], cs[HALF:]
    rot = jnp.concatenate(
        [rope_fwd(kt[DIM * g : DIM * (g + 1)], cos, sin, kgain) for g in range(GROUPS)], axis=0
    ).astype(BF16)
    kvb[0, :t] = dot(ident, rot, NT).astype(BF16)
    kvb[0, t:] = v_ref[...]

    def to_right(s, c):
        part = pl.ds(c * crow, crow)
        return pltpu.make_async_remote_copy(
            src_ref=kvb.at[s - 1, part], dst_ref=kvb.at[s, part],
            send_sem=g_send.at[0, s - 1, c], recv_sem=g_recv.at[0, s - 1, c],
            device_id={"sp": right}, device_id_type=MESH,
        )

    def to_left(s, c):
        part = pl.ds(c * crow, crow)
        return pltpu.make_async_remote_copy(
            src_ref=kvb.at[(n + 1 - s) % n, part], dst_ref=kvb.at[n - s, part],
            send_sem=g_send.at[1, s - 1, c], recv_sem=g_recv.at[1, s - 1, c],
            device_id={"sp": left}, device_id_type=MESH,
        )

    def to_plane(k):
        return pltpu.make_async_remote_copy(
            src_ref=w_all.at[w_rows], dst_ref=w_all.at[w_rows],
            send_sem=w_send.at[k], recv_sem=w_recv.at[k],
            device_id={"dp": (dme + k) % nd}, device_id_type=MESH,
        )

    pl.semaphore_wait(barrier, n - 1 + nd - 1)
    for c in range(CHUNKS):
        to_right(1, c).start()
        to_left(1, c).start()

    def start_w(k, _):
        to_plane(k).start()
        return 0

    lax.fori_loop(1, nd, start_w, 0)

    qbd[...] = jnp.zeros_like(qbd)
    obd[...] = jnp.zeros_like(obd)
    for g in range(GROUPS):
        tr = dot(perm, q_ref[:, KVW * g : KVW * (g + 1)], NT)
        qt[g] = tr
        ot = dot(ident_w, do_ref[:, KVW * g : KVW * (g + 1)], NT).astype(BF16)
        for i in range(PER):
            rows = slice(DIM * i, DIM * (i + 1))
            qr = rope_fwd(tr[rows], cos, sin, qgain).astype(BF16) * jnp.asarray(SCALE, BF16)
            cols = slice(w * g + t * i, w * g + t * (i + 1))
            qbd[DIM * g : DIM * (g + 1), cols] = qr
            obd[DIM * g : DIM * (g + 1), cols] = ot[rows]

    mrun[...] = jnp.full_like(mrun, -jnp.inf)
    lsum[...] = jnp.zeros_like(lsum)
    dsum[...] = jnp.zeros_like(dsum)
    dqt[...] = jnp.zeros_like(dqt)

    def first_pass(slots, step, g):
        cols = slice(w * g, w * (g + 1))
        kb = jnp.concatenate([kvb[r, :t] for r in slots], axis=0)
        vb = jnp.concatenate([kvb[r, t:] for r in slots], axis=0)
        s = dot(kb, qbd[:, cols])
        dp = dot(vb, obd[:, cols])
        m_old = mrun[:, cols]
        m_new = jnp.maximum(m_old, jnp.max(s, axis=0, keepdims=True))
        e = jnp.exp(s - m_new)
        a = jnp.exp(m_old - m_new)
        mrun[:, cols] = m_new
        mj[step, :, cols] = m_new
        lsum[:, cols] = lsum[:, cols] * a + jnp.sum(e, axis=0, keepdims=True)
        dsum[:, cols] = dsum[:, cols] * a + jnp.sum(e * dp, axis=0, keepdims=True)
        for i, r in enumerate(slots):
            e_ref[r, :, cols] = e[t * i : t * (i + 1)]
            dp_ref[r, :, cols] = dp[t * i : t * (i + 1)]

    for g in range(GROUPS):
        first_pass((0,), 0, g)

    for c in range(CHUNKS):
        to_right(1, c).wait_recv()
        if h > 2 or c < 2:
            to_right(2, c).start()
        to_left(1, c).wait_recv()
        if h > 2 or c >= 2:
            to_left(2, c).start()

    def gather_step(s, _):
        for c in range(CHUNKS):
            def receive(copy, s=s, c=c):
                copy(s, c).wait_recv()

            def forward(copy, s=s, c=c):
                copy(s + 1, c).start()

            for copy, whole in ((to_right, c < 2), (to_left, c >= 2)):
                if whole:
                    receive(copy)
                    pl.when(s < h)(functools.partial(forward, copy))
                else:
                    pl.when(s < h)(functools.partial(receive, copy))
                    pl.when(s < h - 1)(functools.partial(forward, copy))
            first_pass((s - 1, n + 1 - s), s - 1, c)
        return 0

    lax.fori_loop(2, h + 1, gather_step, 0)
    for g in range(GROUPS):
        first_pass((h,), h, g)

    for i in range(GROUPS * PER):
        cols = slice(t * i, t * (i + 1))
        qbdt[cols, :] = dot(ident, qbd[:, cols], NT).astype(BF16)
        obdt[cols, :] = dot(ident, obd[:, cols], NT).astype(BF16)
    lsum[...] = 1.0 / lsum[...]
    dsum[...] = dsum[...] * lsum[...]

    def second_pass(slots, step, g, place):
        cols = slice(w * g, w * (g + 1))
        half = slice(HALFW * (g // 2), HALFW * (g // 2 + 1))
        rows = len(slots) * t
        kb = jnp.concatenate([kvb[r, :t] for r in slots], axis=0)
        ktg = dot(ident_w[DIM * g : DIM * (g + 1)], kb, NT).astype(BF16)
        coef = jnp.exp(mj[step, :, cols] - mrun[:, cols]) * lsum[:, cols]
        e = jnp.concatenate([e_ref[r, :, cols] for r in slots], axis=0)
        dp = jnp.concatenate([dp_ref[r, :, cols] for r in slots], axis=0)
        p = e * coef
        ds = (p * (dp - dsum[:, cols])).astype(BF16)
        dv = dot(p.astype(BF16), obdt[cols, half])
        dk = dot(ds, qbdt[cols, half])
        c = 2 * (g // 2)
        if g % 2 == 0:
            acc[place, c, :rows] = dv
            acc[place, c + 1, :rows] = dk
        else:
            acc[place, c, :rows] += dv
            acc[place, c + 1, :rows] += dk
        dqt[DIM * g : DIM * (g + 1)] += dot(ktg, ds)

    def pass_on(d, u, c):
        return pltpu.make_async_remote_copy(
            src_ref=sbuf.at[d, u, c], dst_ref=rbuf.at[d, u, c],
            send_sem=r_send.at[d, u, c], recv_sem=r_recv.at[d, u, c],
            device_id={"sp": left if d else right}, device_id_type=MESH,
        )

    for c in range(CHUNKS):
        rbuf[c % 2, 0, c] = jnp.zeros((t, HALFW), BF16)
    for g in range(GROUPS):
        second_pass((h,), h, g, 0)
        if g % 2 == 1:
            for c in (g - 1, g):
                d = 1 - c % 2
                sbuf[d, 0, c] = acc[0, c, :t].astype(BF16)
                pass_on(d, 0, c).start()
    for g in range(GROUPS):
        second_pass((h + 1, h - 1), h - 1, g, 1)

    def add_and_send(u, c, place):
        for d in range(2):
            def arrived(d=d):
                pass_on(d, u - 1, c).wait_recv()

            if d == 1 - c % 2:
                arrived()
            else:
                pl.when(u > 1)(arrived)
            total = acc[place, c, t * d : t * (d + 1)] + rbuf[d, u - 1, c].astype(F32)
            sbuf[d, u, c] = total.astype(BF16)
            pass_on(d, u, c).start()

    def reduce_step(u, _):
        for c in range(CHUNKS):
            add_and_send(u, c, u % 2)
            second_pass((h + 1 + u, h - 1 - u), h - 1 - u, c, (u + 1) % 2)
        return 0

    lax.fori_loop(1, h - 1, reduce_step, 0)
    last = (h - 1) % 2
    for c in range(CHUNKS):
        add_and_send(h - 1, c, last)
        second_pass((0,), 0, c, 1 - last)

    perm_t = split_pairs(True)
    for g in range(GROUPS):
        y = jnp.concatenate(
            [
                rope_bwd(
                    dqt[DIM * g : DIM * (g + 1), t * i : t * (i + 1)] * SCALE,
                    qt[g, DIM * i : DIM * (i + 1)], cos, sin, qgain,
                )
                for i in range(PER)
            ],
            axis=0,
        ).astype(BF16)
        y = dot(perm_t, y).astype(BF16)
        qg_ref[:, KVW * g : KVW * (g + 1)] = dot(ident, y, NT).astype(BF16)
    width = x_ref.shape[1]
    for i in range(width // HALFW):
        cols = slice(HALFW * i, HALFW * (i + 1))
        xt[cols, :] = dot(eye(HALFW), x_ref[:, cols], NT).astype(BF16)

    whole = []
    for c in range(CHUNKS):
        for d in range(2):
            pass_on(d, h - 1, c).wait_recv()
        whole.append(
            acc[1 - last, c, :t] + rbuf[0, h - 1, c].astype(F32) + rbuf[1, h - 1, c].astype(F32)
        )
    dkt = jnp.transpose(jnp.concatenate([whole[1], whole[3]], axis=1))
    y = jnp.concatenate(
        [
            rope_bwd(dkt[DIM * g : DIM * (g + 1)], kt[DIM * g : DIM * (g + 1)], cos, sin, kgain)
            for g in range(GROUPS)
        ],
        axis=0,
    ).astype(BF16)
    y = dot(perm_t, y).astype(BF16)
    pg = jnp.concatenate(
        [dot(ident, y, NT).astype(BF16), whole[0].astype(BF16), whole[2].astype(BF16)], axis=1
    )

    def to_partner():
        return pltpu.make_async_remote_copy(
            src_ref=wp.at[1 - core], dst_ref=pbuf, send_sem=p_send, recv_sem=p_recv,
            device_id={"dp": dme + 1 - 2 * core}, device_id_type=MESH,
        )

    def to_chip(k):
        return pltpu.make_async_remote_copy(
            src_ref=asend.at[k], dst_ref=arecv.at[k], send_sem=a_send.at[k], recv_sem=a_recv.at[k],
            device_id={"dp": ((chip + k) % chips) * 2 + core}, device_id_type=MESH,
        )

    per_dot = min(8, nd)
    for i in range(nd // per_dot):
        part = dot(xt[wrow * per_dot * i : wrow * per_dot * (i + 1)], pg).astype(BF16)
        for j in range(per_dot):
            o = per_dot * i + j
            wp[o % 2, o // 2] = part[wrow * j : wrow * (j + 1)]
    to_partner().start()

    def wait_w(k, _):
        to_plane(k).wait_recv()
        return 0

    to_partner().wait_recv()

    def send_chip(k, _):
        o = (chip + k) % chips
        asend[k] = (wp[core, o].astype(F32) + pbuf[o].astype(F32)).astype(BF16)
        to_chip(k).start()
        return 0

    lax.fori_loop(1, chips, send_chip, 0)
    lax.fori_loop(1, nd, wait_w, 0)
    for i in range(width // KVW):
        rows = slice(KVW * i, KVW * (i + 1))
        ig_ref[:, rows] = dot(pg, w_all[rows, :], NT).astype(BF16)

    def take_chip(k, total):
        to_chip(k).wait_recv()
        return total + arecv[k].astype(F32)

    mine = wp[core, chip].astype(F32) + pbuf[chip].astype(F32)
    mine = lax.fori_loop(1, chips, take_chip, mine).astype(BF16)

    zrow = zsend.shape[1]
    ncol = 2 * KVW // HALFW
    for i in range(n):
        zsend[i] = mine[zrow * (i // ncol) : zrow * (i // ncol + 1), HALFW * (i % ncol) : HALFW * (i % ncol + 1)]

    def to_depth(k):
        return pltpu.make_async_remote_copy(
            src_ref=zsend.at[(me + k) % n], dst_ref=zrecv.at[k],
            send_sem=z_send.at[k], recv_sem=z_recv.at[k],
            device_id={"sp": (me + k) % n}, device_id_type=MESH,
        )

    def to_all(k):
        return pltpu.make_async_remote_copy(
            src_ref=zall.at[me], dst_ref=zall.at[me],
            send_sem=y_send.at[k], recv_sem=y_recv.at[k],
            device_id={"sp": (me + k) % n}, device_id_type=MESH,
        )

    def start_depth(k, _):
        to_depth(k).start()
        return 0

    def take_depth(k, total):
        to_depth(k).wait_recv()
        return total + zrecv[k].astype(F32)

    def start_all(k, _):
        to_all(k).start()
        return 0

    def wait_all(k, _):
        to_all(k).wait_recv()
        return 0

    lax.fori_loop(1, n, start_depth, 0)
    piece = lax.fori_loop(1, n, take_depth, zsend[me].astype(F32))
    zall[me] = piece.astype(BF16)
    lax.fori_loop(1, n, start_all, 0)
    lax.fori_loop(1, n, wait_all, 0)
    for i in range(n):
        rows = slice(zrow * (i // ncol), zrow * (i // ncol + 1))
        col = i % ncol
        out = kw_ref if col < ncol // 2 else vw_ref
        col = col % (ncol // 2)
        out[rows, HALFW * col : HALFW * (col + 1)] = zall[i].astype(F32)

    def drain_gather(s, _):
        for c in range(CHUNKS):
            to_right(s, c).wait_send()
            to_left(s, c).wait_send()
        return 0

    lax.fori_loop(1, h, drain_gather, 0)
    for c in range(CHUNKS):
        (to_right if c < 2 else to_left)(h, c).wait_send()
        pass_on(1 - c % 2, 0, c).wait_send()

    def drain_reduce(u, _):
        for c in range(CHUNKS):
            pass_on(0, u, c).wait_send()
            pass_on(1, u, c).wait_send()
        return 0

    lax.fori_loop(1, h, drain_reduce, 0)

    def drain_dp(k, _):
        to_plane(k).wait_send()
        return 0

    lax.fori_loop(1, nd, drain_dp, 0)
    to_partner().wait_send()

    def drain_chip(k, _):
        to_chip(k).wait_send()
        return 0

    lax.fori_loop(1, chips, drain_chip, 0)

    def drain_sp(k, _):
        to_depth(k).wait_send()
        to_all(k).wait_send()
        return 0

    lax.fori_loop(1, n, drain_sp, 0)


def tables(n, t):
    pos = np.arange(n * t)
    row = (pos // GRID).astype(np.float32)
    col = (pos % GRID).astype(np.float32)
    m = DIM // 4
    inv = (np.float32(ROPE_BASE) ** (-np.arange(m, dtype=np.float32) / np.float32(m))).astype(np.float32)
    ang = np.concatenate([inv[:, None] * row, inv[:, None] * col], axis=0)
    cs = np.concatenate([np.cos(ang), np.sin(ang)], axis=0).astype(np.float32)
    return np.ascontiguousarray(cs.reshape(2 * HALF, n, t).transpose(1, 0, 2))


def on_device(n, nd, inputs, queries, keys, values, out_grad, query_gain, key_gain, key_matrix, value_matrix):
    t = inputs.shape[1]
    width = inputs.shape[2]
    wrow = key_matrix.shape[0]
    q_all = GROUPS * PER * t
    h = n // 2
    chips = nd // 2
    zrow = wrow * 2 * KVW // HALFW // n
    dma = pltpu.SemaphoreType.DMA
    vmem = pl.BlockSpec(memory_space=pltpu.VMEM)
    shape = jax.ShapeDtypeStruct
    input_grad, query_grad, kw, vw = pl.pallas_call(
        functools.partial(kernel, n, nd),
        out_shape=(
            shape((t, width), BF16),
            shape((t, GROUPS * PER * DIM), BF16),
            shape((wrow, KVW), F32),
            shape((wrow, KVW), F32),
        ),
        in_specs=[vmem] * 9 + [pl.BlockSpec(memory_space=pl.ANY)],
        out_specs=(vmem,) * 4,
        scratch_shapes=[
            pltpu.VMEM((2 * HALF, t), F32),
            pltpu.VMEM((n, 2 * t, KVW), BF16),
            pltpu.VMEM((width, 2 * KVW), BF16),
            pltpu.VMEM((KVW, q_all), BF16),
            pltpu.VMEM((q_all, KVW), BF16),
            pltpu.VMEM((KVW, q_all), BF16),
            pltpu.VMEM((q_all, KVW), BF16),
            pltpu.VMEM((n, t, q_all), F32),
            pltpu.VMEM((n, t, q_all), F32),
            pltpu.VMEM((h + 1, 1, q_all), F32),
            pltpu.VMEM((1, q_all), F32),
            pltpu.VMEM((1, q_all), F32),
            pltpu.VMEM((1, q_all), F32),
            pltpu.VMEM((GROUPS, KVW, t), F32),
            pltpu.VMEM((KVW, t), F32),
            pltpu.VMEM((width, t), BF16),
            pltpu.VMEM((KVW, PER * t), F32),
            pltpu.VMEM((2, CHUNKS, 2 * t, HALFW), F32),
            pltpu.VMEM((2, h, CHUNKS, t, HALFW), BF16),
            pltpu.VMEM((2, h, CHUNKS, t, HALFW), BF16),
            pltpu.VMEM((2, chips, wrow, 2 * KVW), BF16),
            pltpu.VMEM((chips, wrow, 2 * KVW), BF16),
            pltpu.VMEM((chips, wrow, 2 * KVW), BF16),
            pltpu.VMEM((chips, wrow, 2 * KVW), BF16),
            pltpu.VMEM((n, zrow, HALFW), BF16),
            pltpu.VMEM((n, zrow, HALFW), BF16),
            pltpu.VMEM((n, zrow, HALFW), BF16),
            dma,
            dma((2, h, CHUNKS)),
            dma((2, h, CHUNKS)),
            dma((nd,)),
            dma((nd,)),
            dma((2, h, CHUNKS)),
            dma((2, h, CHUNKS)),
            dma,
            dma,
            dma((chips,)),
            dma((chips,)),
            dma((n,)),
            dma((n,)),
            dma((n,)),
            dma((n,)),
        ],
        compiler_params=pltpu.CompilerParams(
            collective_id=0, has_side_effects=True, vmem_limit_bytes=66_000_000
        ),
    )(
        inputs[0], queries[0], keys[0], values[0], out_grad[0],
        query_gain.reshape(1, DIM), key_gain.reshape(1, DIM), key_matrix, value_matrix,
        jnp.asarray(tables(n, t)),
    )
    return input_grad[None], query_grad[None], kw, vw


def solution(mesh):
    row = P("dp", "sp", None)
    return jax.shard_map(
        functools.partial(on_device, mesh.shape["sp"], mesh.shape["dp"]),
        mesh=mesh,
        in_specs=(row, row, row, row, row, P(), P(), P("dp", None), P("dp", None)),
        out_specs=(row, row, P("dp", None), P("dp", None)),
        check_vma=False,
    )
```

```python
import functools

import jax
import jax.numpy as jnp
import numpy as np
from jax import lax
from jax.experimental import pallas as pl
from jax.experimental.pallas import tpu as pltpu
from jax.sharding import PartitionSpec as P

GROUPS = 4
PER = 4
DIM = 64
HALF = 32
GRID = 64
ROPE_BASE = 10000.0
EPS = 0.5
SCALE = 0.125
KVW = GROUPS * DIM
HALFW = 2 * DIM
CHUNKS = 4
PARTS = 4
SUBS = 1
F32 = jnp.float32
BF16 = jnp.bfloat16
MESH = pl.DeviceIdType.MESH

NN = (((1,), (0,)), ((), ()))
NT = (((1,), (1,)), ((), ()))


def dot(a, b, dims=NN):
    return lax.dot_general(a, b, dims, preferred_element_type=F32)


def split_source(shape, axis):
    r = lax.broadcasted_iota(jnp.int32, shape, axis)
    i = r % DIM
    return r - i + jnp.where(i < HALF, 2 * i, 2 * i - (DIM - 1))


def split_pairs(transposed=False):
    axis = 1 if transposed else 0
    c = lax.broadcasted_iota(jnp.int32, (KVW, KVW), 1 - axis)
    return (c == split_source((KVW, KVW), axis)).astype(F32).astype(BF16)


def split_gain(gain):
    c = lax.broadcasted_iota(jnp.int32, (DIM, DIM), 1)
    pick = c == split_source((DIM, DIM), 0)
    return jnp.sum(jnp.where(pick, gain, 0.0), axis=1, keepdims=True)


def eye(n):
    r = lax.broadcasted_iota(jnp.int32, (n, n), 0)
    c = lax.broadcasted_iota(jnp.int32, (n, n), 1)
    return (r == c).astype(F32).astype(BF16)


def inv_rms(a, b):
    ms = (jnp.sum(a * a, axis=0, keepdims=True) + jnp.sum(b * b, axis=0, keepdims=True)) * (1.0 / DIM)
    return lax.rsqrt(ms + EPS)


def rope_fwd(x, cos, sin, gain):
    a, b = x[:HALF], x[HALF:]
    r = inv_rms(a, b)
    a = a * r * gain[:HALF]
    b = b * r * gain[HALF:]
    return jnp.concatenate([a * cos - b * sin, a * sin + b * cos], axis=0)


def rope_bwd(g, x, cos, sin, gain):
    a, b = g[:HALF], g[HALF:]
    ua = (a * cos + b * sin) * gain[:HALF]
    ub = (b * cos - a * sin) * gain[HALF:]
    qa, qb = x[:HALF], x[HALF:]
    r = inv_rms(qa, qb)
    inner = (jnp.sum(ua * qa, axis=0, keepdims=True) + jnp.sum(ub * qb, axis=0, keepdims=True)) * (1.0 / DIM)
    f = r * r * inner
    return jnp.concatenate([r * (ua - qa * f), r * (ub - qb * f)], axis=0)


def kernel(
    n, nd,
    k_ref, v_ref, qgain_ref, kgain_ref, km_ref, vm_ref, x_hbm, q_hbm, do_hbm, tab_ref,
    ig_ref, qg_ref, zall,
    x_ref, q_ref, do_ref,
    cs, kvb, w_all, qbd, qbdt, obd, obdt, e_ref, dp_ref, mj, mrun, lsum, dsum, qt, kt, xt, dqt, acc,
    sbuf, rbuf, wp, pbuf, asend, arecv, zsend, zrecv,
    in_sem, tab_sem, g_send, g_recv, w_send, w_recv, r_send, r_recv, p_send, p_recv, a_send, a_recv,
    z_send, z_recv, y_send, y_recv,
):
    t = q_ref.shape[0]
    w = PER * t
    h = n // 2
    crow = 2 * t // PARTS
    srow = t // SUBS
    wrow = km_ref.shape[0]
    chips = nd // 2
    me = lax.axis_index("sp")
    dme = lax.axis_index("dp")
    core = dme % 2
    chip = dme // 2
    right = (me + 1) % n
    left = (me + n - 1) % n

    def wait_bytes(ref, sem):
        pltpu.make_async_copy(ref, ref, sem).wait()

    table = pltpu.make_async_copy(tab_ref.at[me], cs, tab_sem)
    table.start()
    fetch_q = pltpu.make_async_copy(q_hbm, q_ref, in_sem.at[0])
    fetch_do = pltpu.make_async_copy(do_hbm, do_ref, in_sem.at[1])
    fetch_x = pltpu.make_async_copy(x_hbm, x_ref, in_sem.at[2])
    fetch_q.start()
    fetch_do.start()
    fetch_x.start()
    barrier = pltpu.get_barrier_semaphore()

    def greet_sp(k, _):
        pl.semaphore_signal(barrier, inc=1, device_id={"sp": (me + k) % n}, device_id_type=MESH)
        return 0

    def greet_dp(k, _):
        pl.semaphore_signal(barrier, inc=1, device_id={"dp": (dme + k) % nd}, device_id_type=MESH)
        return 0

    lax.fori_loop(1, n, greet_sp, 0)
    lax.fori_loop(1, nd, greet_dp, 0)

    perm = split_pairs()
    ident = eye(t)
    ident_w = eye(KVW)
    qgain = split_gain(qgain_ref[...])
    kgain = split_gain(kgain_ref[...])
    kt[...] = dot(perm, k_ref[...], NT)
    w_rows = pl.ds(dme * wrow, wrow)
    w_all[w_rows, :KVW] = km_ref[...]
    w_all[w_rows, KVW:] = vm_ref[...]
    table.wait()
    cos, sin = cs[:HALF], cs[HALF:]
    rot = jnp.concatenate(
        [rope_fwd(kt[DIM * g : DIM * (g + 1)], cos, sin, kgain) for g in range(GROUPS)], axis=0
    ).astype(BF16)
    kvb[0, :t] = dot(ident, rot, NT).astype(BF16)
    kvb[0, t:] = v_ref[...]

    def to_right(s, c):
        part = pl.ds(c * crow, crow)
        return pltpu.make_async_remote_copy(
            src_ref=kvb.at[s - 1, part], dst_ref=kvb.at[s, part],
            send_sem=g_send, recv_sem=g_recv.at[0, s - 1, c],
            device_id={"sp": right}, device_id_type=MESH,
        )

    def to_left(s, c):
        part = pl.ds(c * crow, crow)
        return pltpu.make_async_remote_copy(
            src_ref=kvb.at[(n + 1 - s) % n, part], dst_ref=kvb.at[n - s, part],
            send_sem=g_send, recv_sem=g_recv.at[1, s - 1, c],
            device_id={"sp": left}, device_id_type=MESH,
        )

    def to_plane(k):
        return pltpu.make_async_remote_copy(
            src_ref=w_all.at[w_rows], dst_ref=w_all.at[w_rows],
            send_sem=w_send, recv_sem=w_recv,
            device_id={"dp": (dme + k) % nd}, device_id_type=MESH,
        )

    pl.semaphore_wait(barrier, n - 1 + nd - 1)
    for c in range(PARTS):
        to_right(1, c).start()
        to_left(1, c).start()

    def start_w(k, _):
        to_plane(k).start()
        return 0

    lax.fori_loop(1, nd, start_w, 0)

    fetch_q.wait()
    fetch_do.wait()
    qbd[...] = jnp.zeros_like(qbd)
    obd[...] = jnp.zeros_like(obd)
    for g in range(GROUPS):
        tr = dot(perm, q_ref[:, KVW * g : KVW * (g + 1)], NT)
        qt[g] = tr
        ot = dot(ident_w, do_ref[:, KVW * g : KVW * (g + 1)], NT).astype(BF16)
        for i in range(PER):
            rows = slice(DIM * i, DIM * (i + 1))
            qr = rope_fwd(tr[rows], cos, sin, qgain).astype(BF16) * jnp.asarray(SCALE, BF16)
            cols = slice(w * g + t * i, w * g + t * (i + 1))
            qbd[DIM * g : DIM * (g + 1), cols] = qr
            obd[DIM * g : DIM * (g + 1), cols] = ot[rows]

    mrun[...] = jnp.full_like(mrun, -jnp.inf)
    lsum[...] = jnp.zeros_like(lsum)
    dsum[...] = jnp.zeros_like(dsum)
    dqt[...] = jnp.zeros_like(dqt)

    def first_pass(slots, step, g):
        cols = slice(w * g, w * (g + 1))
        kb = jnp.concatenate([kvb[r, :t] for r in slots], axis=0)
        vb = jnp.concatenate([kvb[r, t:] for r in slots], axis=0)
        s = dot(kb, qbd[:, cols])
        dp = dot(vb, obd[:, cols])
        m_old = mrun[:, cols]
        m_new = jnp.maximum(m_old, jnp.max(s, axis=0, keepdims=True))
        e = jnp.exp(s - m_new)
        a = jnp.exp(m_old - m_new)
        mrun[:, cols] = m_new
        mj[step, :, cols] = m_new
        lsum[:, cols] = lsum[:, cols] * a + jnp.sum(e, axis=0, keepdims=True)
        dsum[:, cols] = dsum[:, cols] * a + jnp.sum(e * dp, axis=0, keepdims=True)
        for i, r in enumerate(slots):
            e_ref[r, :, cols] = e[t * i : t * (i + 1)]
            dp_ref[r, :, cols] = dp[t * i : t * (i + 1)]

    for g in range(GROUPS):
        first_pass((0,), 0, g)
    for i in range(GROUPS * PER):
        cols = slice(t * i, t * (i + 1))
        qbdt[cols, :] = dot(ident, qbd[:, cols], NT).astype(BF16)
        obdt[cols, :] = dot(ident, obd[:, cols], NT).astype(BF16)

    for c in range(PARTS):
        to_right(1, c).wait_recv()
        if h > 2 or c < PARTS // 2:
            to_right(2, c).start()
        to_left(1, c).wait_recv()
        if h > 2 or c >= PARTS // 2:
            to_left(2, c).start()

    def gather_step(s, _):
        for c in range(PARTS):
            def receive(copy, s=s, c=c):
                copy(s, c).wait_recv()

            def forward(copy, s=s, c=c):
                copy(s + 1, c).start()

            for copy, whole in ((to_right, c < PARTS // 2), (to_left, c >= PARTS // 2)):
                if whole:
                    receive(copy)
                    pl.when(s < h)(functools.partial(forward, copy))
                else:
                    pl.when(s < h)(functools.partial(receive, copy))
                    pl.when(s < h - 1)(functools.partial(forward, copy))
            first_pass((s - 1, n + 1 - s), s - 1, c)
        return 0

    lax.fori_loop(2, h + 1, gather_step, 0)
    for g in range(GROUPS):
        first_pass((h,), h, g)

    lsum[...] = 1.0 / lsum[...]
    dsum[...] = dsum[...] * lsum[...]

    def second_pass(slots, step, g, place):
        cols = slice(w * g, w * (g + 1))
        half = slice(HALFW * (g // 2), HALFW * (g // 2 + 1))
        rows = len(slots) * t
        kb = jnp.concatenate([kvb[r, :t] for r in slots], axis=0)
        ktg = dot(ident_w[DIM * g : DIM * (g + 1)], kb, NT).astype(BF16)
        coef = jnp.exp(mj[step, :, cols] - mrun[:, cols]) * lsum[:, cols]
        e = jnp.concatenate([e_ref[r, :, cols] for r in slots], axis=0)
        dp = jnp.concatenate([dp_ref[r, :, cols] for r in slots], axis=0)
        p = e * coef
        ds = (p * (dp - dsum[:, cols])).astype(BF16)
        dv = dot(p.astype(BF16), obdt[cols, half])
        dk = dot(ds, qbdt[cols, half])
        c = 2 * (g // 2)
        if g % 2 == 0:
            acc[place, c, :rows] = dv
            acc[place, c + 1, :rows] = dk
        else:
            acc[place, c, :rows] += dv
            acc[place, c + 1, :rows] += dk
        dqt[DIM * g : DIM * (g + 1)] += dot(ktg, ds)

    def pass_on(d, u, c, b):
        part = pl.ds(srow * b, srow)
        return pltpu.make_async_remote_copy(
            src_ref=sbuf.at[d, u, c, part], dst_ref=rbuf.at[d, u, c, part],
            send_sem=r_send, recv_sem=r_recv.at[d, u, c, b],
            device_id={"sp": left if d else right}, device_id_type=MESH,
        )

    for c in range(CHUNKS):
        rbuf[c % 2, 0, c] = jnp.zeros((t, HALFW), BF16)
    for g in range(GROUPS):
        second_pass((h,), h, g, 0)
        if g % 2 == 1:
            for c in (g - 1, g):
                d = 1 - c % 2
                sbuf[d, 0, c] = acc[0, c, :t].astype(BF16)
                for b in range(SUBS):
                    pass_on(d, 0, c, b).start()
    for g in range(GROUPS):
        second_pass((h + 1, h - 1), h - 1, g, 1)

    def add_and_send(u, c, place):
        for b in range(SUBS):
            for d in range(2):
                def arrived(d=d, b=b):
                    pass_on(d, u - 1, c, b).wait_recv()

                if d == 1 - c % 2:
                    arrived()
                else:
                    pl.when(u > 1)(arrived)
                part = slice(srow * b, srow * (b + 1))
                own = acc[place, c, t * d + srow * b : t * d + srow * (b + 1)]
                sbuf[d, u, c, part] = (own + rbuf[d, u - 1, c, part].astype(F32)).astype(BF16)
                pass_on(d, u, c, b).start()

    def reduce_step(u, _):
        for c in range(CHUNKS):
            add_and_send(u, c, u % 2)
            second_pass((h + 1 + u, h - 1 - u), h - 1 - u, c, (u + 1) % 2)
        return 0

    lax.fori_loop(1, h - 1, reduce_step, 0)
    last = (h - 1) % 2
    for c in range(CHUNKS):
        add_and_send(h - 1, c, last)
        second_pass((0,), 0, c, 1 - last)

    perm_t = split_pairs(True)
    for g in range(GROUPS):
        y = jnp.concatenate(
            [
                rope_bwd(
                    dqt[DIM * g : DIM * (g + 1), t * i : t * (i + 1)] * SCALE,
                    qt[g, DIM * i : DIM * (i + 1)], cos, sin, qgain,
                )
                for i in range(PER)
            ],
            axis=0,
        ).astype(BF16)
        y = dot(perm_t, y).astype(BF16)
        qg_ref[:, KVW * g : KVW * (g + 1)] = dot(ident, y, NT).astype(BF16)
    fetch_x.wait()
    width = x_ref.shape[1]
    for i in range(width // HALFW):
        cols = slice(HALFW * i, HALFW * (i + 1))
        xt[cols, :] = dot(eye(HALFW), x_ref[:, cols], NT).astype(BF16)

    whole = []
    for c in range(CHUNKS):
        for b in range(SUBS):
            for d in range(2):
                pass_on(d, h - 1, c, b).wait_recv()
        whole.append(
            acc[1 - last, c, :t] + rbuf[0, h - 1, c].astype(F32) + rbuf[1, h - 1, c].astype(F32)
        )
    dkt = jnp.transpose(jnp.concatenate([whole[1], whole[3]], axis=1))
    y = jnp.concatenate(
        [
            rope_bwd(dkt[DIM * g : DIM * (g + 1)], kt[DIM * g : DIM * (g + 1)], cos, sin, kgain)
            for g in range(GROUPS)
        ],
        axis=0,
    ).astype(BF16)
    y = dot(perm_t, y).astype(BF16)
    pg = jnp.concatenate(
        [dot(ident, y, NT).astype(BF16), whole[0].astype(BF16), whole[2].astype(BF16)], axis=1
    )

    def to_partner():
        return pltpu.make_async_remote_copy(
            src_ref=wp.at[1 - core], dst_ref=pbuf, send_sem=p_send, recv_sem=p_recv,
            device_id={"dp": dme + 1 - 2 * core}, device_id_type=MESH,
        )

    def to_chip(k):
        return pltpu.make_async_remote_copy(
            src_ref=asend.at[k], dst_ref=arecv.at[k], send_sem=a_send, recv_sem=a_recv.at[k],
            device_id={"dp": ((chip + k) % chips) * 2 + core}, device_id_type=MESH,
        )

    per_dot = min(8, nd)
    for i in range(nd // per_dot):
        part = dot(xt[wrow * per_dot * i : wrow * per_dot * (i + 1)], pg).astype(BF16)
        for j in range(per_dot):
            o = per_dot * i + j
            wp[o % 2, o // 2] = part[wrow * j : wrow * (j + 1)]
    to_partner().start()

    to_partner().wait_recv()

    def send_chip(k, _):
        o = (chip + k) % chips
        asend[k] = (wp[core, o].astype(F32) + pbuf[o].astype(F32)).astype(BF16)
        to_chip(k).start()
        return 0

    lax.fori_loop(1, chips, send_chip, 0)
    wait_bytes(w_all.at[pl.ds(0, wrow * (nd - 1))], w_recv)
    for i in range(width // KVW):
        rows = slice(KVW * i, KVW * (i + 1))
        ig_ref[:, rows] = dot(pg, w_all[rows, :], NT).astype(BF16)

    def take_chip(k, total):
        to_chip(k).wait_recv()
        return total + arecv[k].astype(F32)

    mine = wp[core, chip].astype(F32) + pbuf[chip].astype(F32)
    mine = lax.fori_loop(1, chips, take_chip, mine).astype(BF16)

    zrow = zsend.shape[1]
    ncol = 2 * KVW // HALFW
    for i in range(n):
        zsend[i] = mine[zrow * (i // ncol) : zrow * (i // ncol + 1), HALFW * (i % ncol) : HALFW * (i % ncol + 1)]

    def to_depth(k):
        return pltpu.make_async_remote_copy(
            src_ref=zsend.at[(me + k) % n], dst_ref=zrecv.at[k],
            send_sem=z_send, recv_sem=z_recv,
            device_id={"sp": (me + k) % n}, device_id_type=MESH,
        )

    def to_all(k):
        return pltpu.make_async_remote_copy(
            src_ref=zall.at[me], dst_ref=zall.at[me],
            send_sem=y_send, recv_sem=y_recv,
            device_id={"sp": (me + k) % n}, device_id_type=MESH,
        )

    def start_depth(k, _):
        to_depth(k).start()
        return 0

    def take_depth(k, total):
        return total + zrecv[k].astype(F32)

    def start_all(k, _):
        to_all(k).start()
        return 0

    lax.fori_loop(1, n, start_depth, 0)
    wait_bytes(zrecv.at[pl.ds(0, n - 1)], z_recv)
    piece = lax.fori_loop(1, n, take_depth, zsend[me].astype(F32))
    zall[me] = piece.astype(BF16)
    lax.fori_loop(1, n, start_all, 0)
    wait_bytes(zall.at[pl.ds(0, n - 1)], y_recv)
    wait_bytes(kvb.at[pl.ds(0, n - 1)], g_send)
    wait_bytes(w_all.at[pl.ds(0, wrow * (nd - 1))], w_send)
    wait_bytes(sbuf.at[0], r_send)
    wait_bytes(sbuf.at[1, pl.ds(0, h - 1)], r_send)
    to_partner().wait_send()
    wait_bytes(asend.at[pl.ds(0, chips - 1)], a_send)
    wait_bytes(zsend.at[pl.ds(0, n - 1)], z_send)
    wait_bytes(zall.at[pl.ds(0, n - 1)], y_send)


def results(ig, qg, zall, ig_out, qg_out, kw_out, vw_out, kw, vw, sem):
    copies = [pltpu.make_async_copy(ig, ig_out, sem.at[0]), pltpu.make_async_copy(qg, qg_out, sem.at[1])]
    for copy in copies:
        copy.start()
    n, zrow, _ = zall.shape
    ncol = 2 * KVW // HALFW
    for i in range(n):
        rows = slice(zrow * (i // ncol), zrow * (i // ncol + 1))
        col = i % ncol
        out = kw if col < ncol // 2 else vw
        col = col % (ncol // 2)
        out[rows, HALFW * col : HALFW * (col + 1)] = zall[i].astype(F32)
    copies += [pltpu.make_async_copy(kw, kw_out, sem.at[2]), pltpu.make_async_copy(vw, vw_out, sem.at[3])]
    for copy in copies[2:]:
        copy.start()
    for copy in copies:
        copy.wait()


def tables(n, t):
    pos = np.arange(n * t)
    row = (pos // GRID).astype(np.float32)
    col = (pos % GRID).astype(np.float32)
    m = DIM // 4
    inv = (np.float32(ROPE_BASE) ** (-np.arange(m, dtype=np.float32) / np.float32(m))).astype(np.float32)
    ang = np.concatenate([inv[:, None] * row, inv[:, None] * col], axis=0)
    cs = np.concatenate([np.cos(ang), np.sin(ang)], axis=0).astype(np.float32)
    return np.ascontiguousarray(cs.reshape(2 * HALF, n, t).transpose(1, 0, 2))


def on_device(n, nd, inputs, queries, keys, values, out_grad, query_gain, key_gain, key_matrix, value_matrix):
    t = inputs.shape[1]
    width = inputs.shape[2]
    wrow = key_matrix.shape[0]
    q_all = GROUPS * PER * t
    h = n // 2
    chips = nd // 2
    zrow = wrow * 2 * KVW // HALFW // n
    dma = pltpu.SemaphoreType.DMA
    vmem = pl.BlockSpec(memory_space=pltpu.VMEM)
    shape = jax.ShapeDtypeStruct
    anywhere = pl.BlockSpec(memory_space=pl.ANY)
    ig, qg, zall = pl.pallas_call(
        functools.partial(kernel, n, nd),
        out_shape=(
            pltpu.VMEM((t, width), BF16),
            pltpu.VMEM((t, GROUPS * PER * DIM), BF16),
            pltpu.VMEM((n, zrow, HALFW), BF16),
        ),
        in_specs=[vmem] * 6 + [anywhere] * 4,
        out_specs=(vmem,) * 3,
        scratch_shapes=[
            pltpu.VMEM((t, width), BF16),
            pltpu.VMEM((t, GROUPS * PER * DIM), BF16),
            pltpu.VMEM((t, GROUPS * PER * DIM), BF16),
            pltpu.VMEM((2 * HALF, t), F32),
            pltpu.VMEM((n, 2 * t, KVW), BF16),
            pltpu.VMEM((width, 2 * KVW), BF16),
            pltpu.VMEM((KVW, q_all), BF16),
            pltpu.VMEM((q_all, KVW), BF16),
            pltpu.VMEM((KVW, q_all), BF16),
            pltpu.VMEM((q_all, KVW), BF16),
            pltpu.VMEM((n, t, q_all), F32),
            pltpu.VMEM((n, t, q_all), F32),
            pltpu.VMEM((h + 1, 1, q_all), F32),
            pltpu.VMEM((1, q_all), F32),
            pltpu.VMEM((1, q_all), F32),
            pltpu.VMEM((1, q_all), F32),
            pltpu.VMEM((GROUPS, KVW, t), F32),
            pltpu.VMEM((KVW, t), F32),
            pltpu.VMEM((width, t), BF16),
            pltpu.VMEM((KVW, PER * t), F32),
            pltpu.VMEM((2, CHUNKS, 2 * t, HALFW), F32),
            pltpu.VMEM((2, h, CHUNKS, t, HALFW), BF16),
            pltpu.VMEM((2, h, CHUNKS, t, HALFW), BF16),
            pltpu.VMEM((2, chips, wrow, 2 * KVW), BF16),
            pltpu.VMEM((chips, wrow, 2 * KVW), BF16),
            pltpu.VMEM((chips, wrow, 2 * KVW), BF16),
            pltpu.VMEM((chips, wrow, 2 * KVW), BF16),
            pltpu.VMEM((n, zrow, HALFW), BF16),
            pltpu.VMEM((n, zrow, HALFW), BF16),
            dma((3,)),
            dma,
            dma,
            dma((2, h, PARTS)),
            dma,
            dma,
            dma,
            dma((2, h, CHUNKS, SUBS)),
            dma,
            dma,
            dma,
            dma((chips,)),
            dma,
            dma,
            dma,
            dma,
        ],
        compiler_params=pltpu.CompilerParams(
            collective_id=0, has_side_effects=True, vmem_limit_bytes=61_000_000
        ),
    )(
        keys[0], values[0], query_gain.reshape(1, DIM), key_gain.reshape(1, DIM), key_matrix, value_matrix,
        inputs[0], queries[0], out_grad[0], jnp.asarray(tables(n, t)),
    )
    input_grad, query_grad, kw, vw = pl.pallas_call(
        results,
        out_shape=(
            shape((t, width), BF16),
            shape((t, GROUPS * PER * DIM), BF16),
            shape((wrow, KVW), F32),
            shape((wrow, KVW), F32),
        ),
        in_specs=[vmem] * 3,
        out_specs=(anywhere,) * 4,
        scratch_shapes=[pltpu.VMEM((wrow, KVW), F32), pltpu.VMEM((wrow, KVW), F32), dma((4,))],
        compiler_params=pltpu.CompilerParams(vmem_limit_bytes=4 * 1024 * 1024),
    )(ig, qg, zall)
    return input_grad[None], query_grad[None], kw, vw


def solution(mesh):
    row = P("dp", "sp", None)
    return jax.shard_map(
        functools.partial(on_device, mesh.shape["sp"], mesh.shape["dp"]),
        mesh=mesh,
        in_specs=(row, row, row, row, row, P(), P(), P("dp", None), P("dp", None)),
        out_specs=(row, row, P("dp", None), P("dp", None)),
        check_vma=False,
    )
```

```python
import functools

import jax
import jax.numpy as jnp
import numpy as np
from jax import lax
from jax.experimental import pallas as pl
from jax.experimental.pallas import tpu as pltpu
from jax.sharding import PartitionSpec as P

GROUPS = 4
PER = 4
DIM = 64
HALF = 32
GRID = 64
ROPE_BASE = 10000.0
EPS = 0.5
SCALE = 0.125
KVW = GROUPS * DIM
HALFW = 2 * DIM
CHUNKS = 4
PARTS = 4
SUBS = 1
F32 = jnp.float32
BF16 = jnp.bfloat16
MESH = pl.DeviceIdType.MESH

NN = (((1,), (0,)), ((), ()))
NT = (((1,), (1,)), ((), ()))


def dot(a, b, dims=NN):
    return lax.dot_general(a, b, dims, preferred_element_type=F32)


def split_source(shape, axis):
    r = lax.broadcasted_iota(jnp.int32, shape, axis)
    i = r % DIM
    return r - i + jnp.where(i < HALF, 2 * i, 2 * i - (DIM - 1))


def split_pairs(transposed=False):
    axis = 1 if transposed else 0
    c = lax.broadcasted_iota(jnp.int32, (KVW, KVW), 1 - axis)
    return (c == split_source((KVW, KVW), axis)).astype(F32).astype(BF16)


def split_gain(gain):
    c = lax.broadcasted_iota(jnp.int32, (DIM, DIM), 1)
    pick = c == split_source((DIM, DIM), 0)
    return jnp.sum(jnp.where(pick, gain, 0.0), axis=1, keepdims=True)


def eye(n):
    r = lax.broadcasted_iota(jnp.int32, (n, n), 0)
    c = lax.broadcasted_iota(jnp.int32, (n, n), 1)
    return (r == c).astype(F32).astype(BF16)


def inv_rms(a, b):
    ms = (jnp.sum(a * a, axis=0, keepdims=True) + jnp.sum(b * b, axis=0, keepdims=True)) * (1.0 / DIM)
    return lax.rsqrt(ms + EPS)


def rope_fwd(x, cos, sin, gain):
    a, b = x[:HALF], x[HALF:]
    r = inv_rms(a, b)
    a = a * r * gain[:HALF]
    b = b * r * gain[HALF:]
    return jnp.concatenate([a * cos - b * sin, a * sin + b * cos], axis=0)


def rope_bwd(g, x, cos, sin, gain):
    a, b = g[:HALF], g[HALF:]
    ua = (a * cos + b * sin) * gain[:HALF]
    ub = (b * cos - a * sin) * gain[HALF:]
    qa, qb = x[:HALF], x[HALF:]
    r = inv_rms(qa, qb)
    inner = (jnp.sum(ua * qa, axis=0, keepdims=True) + jnp.sum(ub * qb, axis=0, keepdims=True)) * (1.0 / DIM)
    f = r * r * inner
    return jnp.concatenate([r * (ua - qa * f), r * (ub - qb * f)], axis=0)


def kernel(
    n, nd,
    k_ref, v_ref, qgain_ref, kgain_ref, km_ref, vm_ref, x_hbm, q_hbm, do_hbm, tab_ref,
    ig_ref, qg_ref, zall,
    x_ref, q_ref, do_ref, kx, own, ig_s, qg_s,
    cs, kvb, w_all, qbd, qbdt, obd, obdt, e_ref, dp_ref, mj, mrun, lsum, dsum, qt, kt, xt, dqt, acc,
    sbuf, rbuf, wp, pbuf, asend, arecv, zsend, zrecv,
    in_sem, swap_send, back_recv, tab_sem, g_send, g_recv, w_send, w_recv, r_send, r_recv, p_send, p_recv, a_send, a_recv,
    z_send, z_recv, y_send, y_recv,
):
    t = q_ref.shape[0]
    w = PER * t
    h = n // 2
    crow = 2 * t // PARTS
    srow = t // SUBS
    wrow = km_ref.shape[0]
    chips = nd // 2
    me = lax.axis_index("sp")
    dme = lax.axis_index("dp")
    core = dme % 2
    chip = dme // 2
    right = (me + 1) % n
    left = (me + n - 1) % n
    mate = dme + 1 - 2 * core
    odd = me % 2 == 1
    even = me % 2 == 0
    first_dp = dme + (1 - me % 2) * (1 - 2 * core)

    def wait_bytes(ref, sem):
        pltpu.make_async_copy(ref, ref, sem).wait()

    table = pltpu.make_async_copy(tab_ref.at[me], cs, tab_sem)
    table.start()
    fetch_q = pltpu.make_async_copy(q_hbm, q_ref, in_sem.at[0])
    fetch_do = pltpu.make_async_copy(do_hbm, do_ref, in_sem.at[1])
    fetch_x = pltpu.make_async_copy(x_hbm, x_ref, in_sem.at[2])

    @pl.when(even)
    def _():
        fetch_q.start()
        fetch_do.start()
        fetch_x.start()

    def to_mate(i, src, dst, recv_sem):
        return pltpu.make_async_remote_copy(
            src_ref=src, dst_ref=dst, send_sem=swap_send.at[i], recv_sem=recv_sem,
            device_id={"dp": mate}, device_id_type=MESH,
        )

    swap_kv = to_mate(0, own, kvb.at[0], in_sem.at[3])
    swaps = [
        swap_kv,
        to_mate(1, q_hbm, q_ref, in_sem.at[0]),
        to_mate(2, do_hbm, do_ref, in_sem.at[1]),
        to_mate(3, k_ref, kx, in_sem.at[4]),
        to_mate(4, x_hbm, x_ref, in_sem.at[2]),
    ]
    backs = [to_mate(5, qg_s, qg_ref, back_recv.at[0]), to_mate(6, ig_s, ig_ref, back_recv.at[1])]
    barrier = pltpu.get_barrier_semaphore()

    def greet_sp(k, _):
        pl.semaphore_signal(barrier, inc=1, device_id={"sp": (me + k) % n}, device_id_type=MESH)
        return 0

    def greet_dp(k, _):
        pl.semaphore_signal(barrier, inc=1, device_id={"dp": (dme + k) % nd}, device_id_type=MESH)
        return 0

    lax.fori_loop(1, n, greet_sp, 0)
    lax.fori_loop(1, nd, greet_dp, 0)
    for side in (left, right):
        pl.semaphore_signal(barrier, inc=1, device_id={"sp": side, "dp": mate}, device_id_type=MESH)

    perm = split_pairs()
    ident = eye(t)
    ident_w = eye(KVW)
    qgain = split_gain(qgain_ref[...])
    kgain = split_gain(kgain_ref[...])
    kt[...] = dot(perm, k_ref[...], NT)
    w_rows = pl.ds(dme * wrow, wrow)
    w_all[w_rows, :KVW] = km_ref[...]
    w_all[w_rows, KVW:] = vm_ref[...]
    table.wait()
    cos, sin = cs[:HALF], cs[HALF:]
    rot = jnp.concatenate(
        [rope_fwd(kt[DIM * g : DIM * (g + 1)], cos, sin, kgain) for g in range(GROUPS)], axis=0
    ).astype(BF16)
    own[:t] = dot(ident, rot, NT).astype(BF16)
    own[t:] = v_ref[...]

    @pl.when(even)
    def _():
        kvb[0] = own[...]

    def to_right(s, c):
        part = pl.ds(c * crow, crow)
        return pltpu.make_async_remote_copy(
            src_ref=kvb.at[s - 1, part], dst_ref=kvb.at[s, part],
            send_sem=g_send, recv_sem=g_recv.at[0, s - 1, c],
            device_id={"sp": right, "dp": mate}, device_id_type=MESH,
        )

    def to_left(s, c):
        part = pl.ds(c * crow, crow)
        return pltpu.make_async_remote_copy(
            src_ref=kvb.at[(n + 1 - s) % n, part], dst_ref=kvb.at[n - s, part],
            send_sem=g_send, recv_sem=g_recv.at[1, s - 1, c],
            device_id={"sp": left, "dp": mate}, device_id_type=MESH,
        )

    def first_hop(c, d):
        part = pl.ds(c * crow, crow)
        return pltpu.make_async_remote_copy(
            src_ref=own.at[part], dst_ref=kvb.at[n - 1 if d else 1, part],
            send_sem=g_send, recv_sem=g_recv.at[d, 0, c],
            device_id={"sp": left if d else right, "dp": first_dp}, device_id_type=MESH,
        )

    def to_plane(k):
        return pltpu.make_async_remote_copy(
            src_ref=w_all.at[w_rows], dst_ref=w_all.at[w_rows],
            send_sem=w_send, recv_sem=w_recv,
            device_id={"dp": (dme + k) % nd}, device_id_type=MESH,
        )

    pl.semaphore_wait(barrier, n - 1 + nd - 1 + 2)
    for c in range(PARTS):
        first_hop(c, 0).start()
        first_hop(c, 1).start()

    @pl.when(odd)
    def _():
        for copy in swaps:
            copy.start()


    def start_w(k, _):
        to_plane(k).start()
        return 0

    lax.fori_loop(1, nd, start_w, 0)

    fetch_q.wait()
    fetch_do.wait()
    qbd[...] = jnp.zeros_like(qbd)
    obd[...] = jnp.zeros_like(obd)
    for g in range(GROUPS):
        tr = dot(perm, q_ref[:, KVW * g : KVW * (g + 1)], NT)
        qt[g] = tr
        ot = dot(ident_w, do_ref[:, KVW * g : KVW * (g + 1)], NT).astype(BF16)
        for i in range(PER):
            rows = slice(DIM * i, DIM * (i + 1))
            qr = rope_fwd(tr[rows], cos, sin, qgain).astype(BF16) * jnp.asarray(SCALE, BF16)
            cols = slice(w * g + t * i, w * g + t * (i + 1))
            qbd[DIM * g : DIM * (g + 1), cols] = qr
            obd[DIM * g : DIM * (g + 1), cols] = ot[rows]

    mrun[...] = jnp.full_like(mrun, -jnp.inf)
    lsum[...] = jnp.zeros_like(lsum)
    dsum[...] = jnp.zeros_like(dsum)
    dqt[...] = jnp.zeros_like(dqt)

    def first_pass(slots, step, g):
        cols = slice(w * g, w * (g + 1))
        kb = jnp.concatenate([kvb[r, :t] for r in slots], axis=0)
        vb = jnp.concatenate([kvb[r, t:] for r in slots], axis=0)
        s = dot(kb, qbd[:, cols])
        dp = dot(vb, obd[:, cols])
        m_old = mrun[:, cols]
        m_new = jnp.maximum(m_old, jnp.max(s, axis=0, keepdims=True))
        e = jnp.exp(s - m_new)
        a = jnp.exp(m_old - m_new)
        mrun[:, cols] = m_new
        mj[step, :, cols] = m_new
        lsum[:, cols] = lsum[:, cols] * a + jnp.sum(e, axis=0, keepdims=True)
        dsum[:, cols] = dsum[:, cols] * a + jnp.sum(e * dp, axis=0, keepdims=True)
        for i, r in enumerate(slots):
            e_ref[r, :, cols] = e[t * i : t * (i + 1)]
            dp_ref[r, :, cols] = dp[t * i : t * (i + 1)]

    pl.when(odd)(swap_kv.wait_recv)
    for g in range(GROUPS):
        first_pass((0,), 0, g)
    for i in range(GROUPS * PER):
        cols = slice(t * i, t * (i + 1))
        qbdt[cols, :] = dot(ident, qbd[:, cols], NT).astype(BF16)
        obdt[cols, :] = dot(ident, obd[:, cols], NT).astype(BF16)

    for c in range(PARTS):
        to_right(1, c).wait_recv()
        if h > 2 or c < PARTS // 2:
            to_right(2, c).start()
        to_left(1, c).wait_recv()
        if h > 2 or c >= PARTS // 2:
            to_left(2, c).start()

    def gather_step(s, _):
        for c in range(PARTS):
            def receive(copy, s=s, c=c):
                copy(s, c).wait_recv()

            def forward(copy, s=s, c=c):
                copy(s + 1, c).start()

            for copy, whole in ((to_right, c < PARTS // 2), (to_left, c >= PARTS // 2)):
                if whole:
                    receive(copy)
                    pl.when(s < h)(functools.partial(forward, copy))
                else:
                    pl.when(s < h)(functools.partial(receive, copy))
                    pl.when(s < h - 1)(functools.partial(forward, copy))
            first_pass((s - 1, n + 1 - s), s - 1, c)
        return 0

    lax.fori_loop(2, h + 1, gather_step, 0)
    for g in range(GROUPS):
        first_pass((h,), h, g)

    lsum[...] = 1.0 / lsum[...]
    dsum[...] = dsum[...] * lsum[...]

    def second_pass(slots, step, g, place):
        cols = slice(w * g, w * (g + 1))
        half = slice(HALFW * (g // 2), HALFW * (g // 2 + 1))
        rows = len(slots) * t
        kb = jnp.concatenate([kvb[r, :t] for r in slots], axis=0)
        ktg = dot(ident_w[DIM * g : DIM * (g + 1)], kb, NT).astype(BF16)
        coef = jnp.exp(mj[step, :, cols] - mrun[:, cols]) * lsum[:, cols]
        e = jnp.concatenate([e_ref[r, :, cols] for r in slots], axis=0)
        dp = jnp.concatenate([dp_ref[r, :, cols] for r in slots], axis=0)
        p = e * coef
        ds = (p * (dp - dsum[:, cols])).astype(BF16)
        dv = dot(p.astype(BF16), obdt[cols, half])
        dk = dot(ds, qbdt[cols, half])
        c = 2 * (g // 2)
        if g % 2 == 0:
            acc[place, c, :rows] = dv
            acc[place, c + 1, :rows] = dk
        else:
            acc[place, c, :rows] += dv
            acc[place, c + 1, :rows] += dk
        dqt[DIM * g : DIM * (g + 1)] += dot(ktg, ds)

    def pass_on(d, u, c, b):
        part = pl.ds(srow * b, srow)
        return pltpu.make_async_remote_copy(
            src_ref=sbuf.at[d, u, c, part], dst_ref=rbuf.at[d, u, c, part],
            send_sem=r_send, recv_sem=r_recv.at[d, u, c, b],
            device_id={"sp": left if d else right, "dp": mate}, device_id_type=MESH,
        )

    for c in range(CHUNKS):
        rbuf[c % 2, 0, c] = jnp.zeros((t, HALFW), BF16)
    for g in range(GROUPS):
        second_pass((h,), h, g, 0)
        if g % 2 == 1:
            for c in (g - 1, g):
                d = 1 - c % 2
                sbuf[d, 0, c] = acc[0, c, :t].astype(BF16)
                for b in range(SUBS):
                    pass_on(d, 0, c, b).start()
    for g in range(GROUPS):
        second_pass((h + 1, h - 1), h - 1, g, 1)

    def add_and_send(u, c, place):
        for b in range(SUBS):
            for d in range(2):
                def arrived(d=d, b=b):
                    pass_on(d, u - 1, c, b).wait_recv()

                if d == 1 - c % 2:
                    arrived()
                else:
                    pl.when(u > 1)(arrived)
                part = slice(srow * b, srow * (b + 1))
                own = acc[place, c, t * d + srow * b : t * d + srow * (b + 1)]
                sbuf[d, u, c, part] = (own + rbuf[d, u - 1, c, part].astype(F32)).astype(BF16)
                pass_on(d, u, c, b).start()

    def reduce_step(u, _):
        for c in range(CHUNKS):
            add_and_send(u, c, u % 2)
            second_pass((h + 1 + u, h - 1 - u), h - 1 - u, c, (u + 1) % 2)
        return 0

    lax.fori_loop(1, h - 1, reduce_step, 0)
    last = (h - 1) % 2
    for c in range(CHUNKS):
        add_and_send(h - 1, c, last)
        second_pass((0,), 0, c, 1 - last)

    perm_t = split_pairs(True)
    for g in range(GROUPS):
        y = jnp.concatenate(
            [
                rope_bwd(
                    dqt[DIM * g : DIM * (g + 1), t * i : t * (i + 1)] * SCALE,
                    qt[g, DIM * i : DIM * (i + 1)], cos, sin, qgain,
                )
                for i in range(PER)
            ],
            axis=0,
        ).astype(BF16)
        y = dot(perm_t, y).astype(BF16)
        qg_s[:, KVW * g : KVW * (g + 1)] = dot(ident, y, NT).astype(BF16)
    pl.when(odd)(backs[0].start)
    fetch_x.wait()

    @pl.when(odd)
    def _():
        swaps[3].wait_recv()
        kt[...] = dot(perm, kx[...], NT)

    width = x_ref.shape[1]
    for i in range(width // HALFW):
        cols = slice(HALFW * i, HALFW * (i + 1))
        xt[cols, :] = dot(eye(HALFW), x_ref[:, cols], NT).astype(BF16)

    whole = []
    for c in range(CHUNKS):
        for b in range(SUBS):
            for d in range(2):
                pass_on(d, h - 1, c, b).wait_recv()
        whole.append(
            acc[1 - last, c, :t] + rbuf[0, h - 1, c].astype(F32) + rbuf[1, h - 1, c].astype(F32)
        )
    dkt = jnp.transpose(jnp.concatenate([whole[1], whole[3]], axis=1))
    y = jnp.concatenate(
        [
            rope_bwd(dkt[DIM * g : DIM * (g + 1)], kt[DIM * g : DIM * (g + 1)], cos, sin, kgain)
            for g in range(GROUPS)
        ],
        axis=0,
    ).astype(BF16)
    y = dot(perm_t, y).astype(BF16)
    pg = jnp.concatenate(
        [dot(ident, y, NT).astype(BF16), whole[0].astype(BF16), whole[2].astype(BF16)], axis=1
    )

    def to_partner():
        return pltpu.make_async_remote_copy(
            src_ref=wp.at[1 - core], dst_ref=pbuf, send_sem=p_send, recv_sem=p_recv,
            device_id={"dp": dme + 1 - 2 * core}, device_id_type=MESH,
        )

    def to_chip(k):
        return pltpu.make_async_remote_copy(
            src_ref=asend.at[k], dst_ref=arecv.at[k], send_sem=a_send, recv_sem=a_recv.at[k],
            device_id={"dp": ((chip + k) % chips) * 2 + core}, device_id_type=MESH,
        )

    per_dot = min(8, nd)
    for i in range(nd // per_dot):
        part = dot(xt[wrow * per_dot * i : wrow * per_dot * (i + 1)], pg).astype(BF16)
        for j in range(per_dot):
            o = per_dot * i + j
            wp[o % 2, o // 2] = part[wrow * j : wrow * (j + 1)]
    to_partner().start()

    to_partner().wait_recv()

    def send_chip(k, _):
        o = (chip + k) % chips
        asend[k] = (wp[core, o].astype(F32) + pbuf[o].astype(F32)).astype(BF16)
        to_chip(k).start()
        return 0

    lax.fori_loop(1, chips, send_chip, 0)
    wait_bytes(w_all.at[pl.ds(0, wrow * (nd - 1))], w_recv)
    for i in range(width // KVW):
        rows = slice(KVW * i, KVW * (i + 1))
        ig_s[:, rows] = dot(pg, w_all[rows, :], NT).astype(BF16)
    pl.when(odd)(backs[1].start)

    @pl.when(even)
    def _():
        qg_ref[...] = qg_s[...]
        ig_ref[...] = ig_s[...]


    def take_chip(k, total):
        to_chip(k).wait_recv()
        return total + arecv[k].astype(F32)

    mine = wp[core, chip].astype(F32) + pbuf[chip].astype(F32)
    mine = lax.fori_loop(1, chips, take_chip, mine).astype(BF16)

    zrow = zsend.shape[1]
    ncol = 2 * KVW // HALFW
    for i in range(n):
        zsend[i] = mine[zrow * (i // ncol) : zrow * (i // ncol + 1), HALFW * (i % ncol) : HALFW * (i % ncol + 1)]

    def to_depth(k):
        return pltpu.make_async_remote_copy(
            src_ref=zsend.at[(me + k) % n], dst_ref=zrecv.at[k],
            send_sem=z_send, recv_sem=z_recv,
            device_id={"sp": (me + k) % n}, device_id_type=MESH,
        )

    def to_all(k):
        return pltpu.make_async_remote_copy(
            src_ref=zall.at[me], dst_ref=zall.at[me],
            send_sem=y_send, recv_sem=y_recv,
            device_id={"sp": (me + k) % n}, device_id_type=MESH,
        )

    def start_depth(k, _):
        to_depth(k).start()
        return 0

    def take_depth(k, total):
        return total + zrecv[k].astype(F32)

    def start_all(k, _):
        to_all(k).start()
        return 0

    lax.fori_loop(1, n, start_depth, 0)
    wait_bytes(zrecv.at[pl.ds(0, n - 1)], z_recv)
    piece = lax.fori_loop(1, n, take_depth, zsend[me].astype(F32))
    zall[me] = piece.astype(BF16)
    lax.fori_loop(1, n, start_all, 0)
    wait_bytes(zall.at[pl.ds(0, n - 1)], y_recv)
    @pl.when(odd)
    def _():
        for copy in backs:
            copy.wait_recv()
        for copy in swaps + backs:
            copy.wait_send()

    wait_bytes(kvb.at[pl.ds(0, n - 1)], g_send)
    wait_bytes(w_all.at[pl.ds(0, wrow * (nd - 1))], w_send)
    wait_bytes(sbuf.at[0], r_send)
    wait_bytes(sbuf.at[1, pl.ds(0, h - 1)], r_send)
    to_partner().wait_send()
    wait_bytes(asend.at[pl.ds(0, chips - 1)], a_send)
    wait_bytes(zsend.at[pl.ds(0, n - 1)], z_send)
    wait_bytes(zall.at[pl.ds(0, n - 1)], y_send)


def results(ig, qg, zall, ig_out, qg_out, kw_out, vw_out, kw, vw, sem):
    copies = [pltpu.make_async_copy(ig, ig_out, sem.at[0]), pltpu.make_async_copy(qg, qg_out, sem.at[1])]
    for copy in copies:
        copy.start()
    n, zrow, _ = zall.shape
    ncol = 2 * KVW // HALFW
    for i in range(n):
        rows = slice(zrow * (i // ncol), zrow * (i // ncol + 1))
        col = i % ncol
        out = kw if col < ncol // 2 else vw
        col = col % (ncol // 2)
        out[rows, HALFW * col : HALFW * (col + 1)] = zall[i].astype(F32)
    copies += [pltpu.make_async_copy(kw, kw_out, sem.at[2]), pltpu.make_async_copy(vw, vw_out, sem.at[3])]
    for copy in copies[2:]:
        copy.start()
    for copy in copies:
        copy.wait()


def tables(n, t):
    pos = np.arange(n * t)
    row = (pos // GRID).astype(np.float32)
    col = (pos % GRID).astype(np.float32)
    m = DIM // 4
    inv = (np.float32(ROPE_BASE) ** (-np.arange(m, dtype=np.float32) / np.float32(m))).astype(np.float32)
    ang = np.concatenate([inv[:, None] * row, inv[:, None] * col], axis=0)
    cs = np.concatenate([np.cos(ang), np.sin(ang)], axis=0).astype(np.float32)
    return np.ascontiguousarray(cs.reshape(2 * HALF, n, t).transpose(1, 0, 2))


def on_device(n, nd, inputs, queries, keys, values, out_grad, query_gain, key_gain, key_matrix, value_matrix):
    t = inputs.shape[1]
    width = inputs.shape[2]
    wrow = key_matrix.shape[0]
    q_all = GROUPS * PER * t
    h = n // 2
    chips = nd // 2
    zrow = wrow * 2 * KVW // HALFW // n
    dma = pltpu.SemaphoreType.DMA
    vmem = pl.BlockSpec(memory_space=pltpu.VMEM)
    shape = jax.ShapeDtypeStruct
    anywhere = pl.BlockSpec(memory_space=pl.ANY)
    ig, qg, zall = pl.pallas_call(
        functools.partial(kernel, n, nd),
        out_shape=(
            pltpu.VMEM((t, width), BF16),
            pltpu.VMEM((t, GROUPS * PER * DIM), BF16),
            pltpu.VMEM((n, zrow, HALFW), BF16),
        ),
        in_specs=[vmem] * 6 + [anywhere] * 4,
        out_specs=(vmem,) * 3,
        scratch_shapes=[
            pltpu.VMEM((t, width), BF16),
            pltpu.VMEM((t, GROUPS * PER * DIM), BF16),
            pltpu.VMEM((t, GROUPS * PER * DIM), BF16),
            pltpu.VMEM((t, KVW), BF16),
            pltpu.VMEM((2 * t, KVW), BF16),
            pltpu.VMEM((t, width), BF16),
            pltpu.VMEM((t, GROUPS * PER * DIM), BF16),
            pltpu.VMEM((2 * HALF, t), F32),
            pltpu.VMEM((n, 2 * t, KVW), BF16),
            pltpu.VMEM((width, 2 * KVW), BF16),
            pltpu.VMEM((KVW, q_all), BF16),
            pltpu.VMEM((q_all, KVW), BF16),
            pltpu.VMEM((KVW, q_all), BF16),
            pltpu.VMEM((q_all, KVW), BF16),
            pltpu.VMEM((n, t, q_all), F32),
            pltpu.VMEM((n, t, q_all), F32),
            pltpu.VMEM((h + 1, 1, q_all), F32),
            pltpu.VMEM((1, q_all), F32),
            pltpu.VMEM((1, q_all), F32),
            pltpu.VMEM((1, q_all), F32),
            pltpu.VMEM((GROUPS, KVW, t), F32),
            pltpu.VMEM((KVW, t), F32),
            pltpu.VMEM((width, t), BF16),
            pltpu.VMEM((KVW, PER * t), F32),
            pltpu.VMEM((2, CHUNKS, 2 * t, HALFW), F32),
            pltpu.VMEM((2, h, CHUNKS, t, HALFW), BF16),
            pltpu.VMEM((2, h, CHUNKS, t, HALFW), BF16),
            pltpu.VMEM((2, chips, wrow, 2 * KVW), BF16),
            pltpu.VMEM((chips, wrow, 2 * KVW), BF16),
            pltpu.VMEM((chips, wrow, 2 * KVW), BF16),
            pltpu.VMEM((chips, wrow, 2 * KVW), BF16),
            pltpu.VMEM((n, zrow, HALFW), BF16),
            pltpu.VMEM((n, zrow, HALFW), BF16),
            dma((5,)),
            dma((7,)),
            dma((2,)),
            dma,
            dma,
            dma((2, h, PARTS)),
            dma,
            dma,
            dma,
            dma((2, h, CHUNKS, SUBS)),
            dma,
            dma,
            dma,
            dma((chips,)),
            dma,
            dma,
            dma,
            dma,
        ],
        compiler_params=pltpu.CompilerParams(
            collective_id=0, has_side_effects=True, vmem_limit_bytes=61_000_000
        ),
    )(
        keys[0], values[0], query_gain.reshape(1, DIM), key_gain.reshape(1, DIM), key_matrix, value_matrix,
        inputs[0], queries[0], out_grad[0], jnp.asarray(tables(n, t)),
    )
    input_grad, query_grad, kw, vw = pl.pallas_call(
        results,
        out_shape=(
            shape((t, width), BF16),
            shape((t, GROUPS * PER * DIM), BF16),
            shape((wrow, KVW), F32),
            shape((wrow, KVW), F32),
        ),
        in_specs=[vmem] * 3,
        out_specs=(anywhere,) * 4,
        scratch_shapes=[pltpu.VMEM((wrow, KVW), F32), pltpu.VMEM((wrow, KVW), F32), dma((4,))],
        compiler_params=pltpu.CompilerParams(vmem_limit_bytes=4 * 1024 * 1024),
    )(ig, qg, zall)
    return input_grad[None], query_grad[None], kw, vw


def solution(mesh):
    row = P("dp", "sp", None)
    return jax.shard_map(
        functools.partial(on_device, mesh.shape["sp"], mesh.shape["dp"]),
        mesh=mesh,
        in_specs=(row, row, row, row, row, P(), P(), P("dp", None), P("dp", None)),
        out_specs=(row, row, P("dp", None), P("dp", None)),
        check_vma=False,
    )
```

```python
import functools

import jax
import jax.numpy as jnp
import numpy as np
from jax import lax
from jax.experimental import pallas as pl
from jax.experimental.pallas import tpu as pltpu
from jax.sharding import PartitionSpec as P

GROUPS = 4
PER = 4
DIM = 64
HALF = 32
GRID = 64
ROPE_BASE = 10000.0
EPS = 0.5
SCALE = 0.125
KVW = GROUPS * DIM
HALFW = 2 * DIM
CHUNKS = 4
PARTS = 4
SUBS = 1
F32 = jnp.float32
BF16 = jnp.bfloat16
MESH = pl.DeviceIdType.MESH

NN = (((1,), (0,)), ((), ()))
NT = (((1,), (1,)), ((), ()))


def dot(a, b, dims=NN):
    return lax.dot_general(a, b, dims, preferred_element_type=F32)


def split_source(shape, axis):
    r = lax.broadcasted_iota(jnp.int32, shape, axis)
    i = r % DIM
    return r - i + jnp.where(i < HALF, 2 * i, 2 * i - (DIM - 1))


def split_pairs(transposed=False):
    axis = 1 if transposed else 0
    c = lax.broadcasted_iota(jnp.int32, (KVW, KVW), 1 - axis)
    return (c == split_source((KVW, KVW), axis)).astype(F32).astype(BF16)


def split_gain(gain):
    c = lax.broadcasted_iota(jnp.int32, (DIM, DIM), 1)
    pick = c == split_source((DIM, DIM), 0)
    return jnp.sum(jnp.where(pick, gain, 0.0), axis=1, keepdims=True)


def eye(n):
    r = lax.broadcasted_iota(jnp.int32, (n, n), 0)
    c = lax.broadcasted_iota(jnp.int32, (n, n), 1)
    return (r == c).astype(F32).astype(BF16)


def inv_rms(a, b):
    ms = (jnp.sum(a * a, axis=0, keepdims=True) + jnp.sum(b * b, axis=0, keepdims=True)) * (1.0 / DIM)
    return lax.rsqrt(ms + EPS)


def rope_fwd(x, cos, sin, gain):
    a, b = x[:HALF], x[HALF:]
    r = inv_rms(a, b)
    a = a * r * gain[:HALF]
    b = b * r * gain[HALF:]
    return jnp.concatenate([a * cos - b * sin, a * sin + b * cos], axis=0)


def rope_bwd(g, x, cos, sin, gain):
    a, b = g[:HALF], g[HALF:]
    ua = (a * cos + b * sin) * gain[:HALF]
    ub = (b * cos - a * sin) * gain[HALF:]
    qa, qb = x[:HALF], x[HALF:]
    r = inv_rms(qa, qb)
    inner = (jnp.sum(ua * qa, axis=0, keepdims=True) + jnp.sum(ub * qb, axis=0, keepdims=True)) * (1.0 / DIM)
    f = r * r * inner
    return jnp.concatenate([r * (ua - qa * f), r * (ub - qb * f)], axis=0)


def kernel(
    n, nd,
    k_hbm, v_hbm, qgain_ref, kgain_ref, km_hbm, vm_hbm, x_hbm, q_hbm, do_hbm, tab_ref,
    ig_ref, qg_ref, zall,
    k_ref, v_ref, km_ref, vm_ref, xx, q_ref, do_ref, kx, own, ig_s, qg_s,
    cs, kvb, w_all, qbd, qbdt, obd, obdt, e_ref, dp_ref, mj, mrun, lsum, dsum, qt, kt, xt, dqt, acc,
    sbuf, rbuf, pgb, asend, arecv, zsend, zrecv,
    first_sem, in_sem, swap_send, back_recv, tab_sem, g_send, g_recv, w_send, w_recv, r_send, r_recv, a_send, a_recv,
    z_send, z_recv, y_send, y_recv, plane,
):
    t = q_ref.shape[0]
    w = PER * t
    h = n // 2
    crow = 2 * t // PARTS
    srow = t // SUBS
    wrow = km_ref.shape[0]
    chips = nd // 2
    me = lax.axis_index("sp")
    dme = lax.axis_index("dp")
    core = dme % 2
    chip = dme // 2
    right = (me + 1) % n
    left = (me + n - 1) % n
    mate = dme + 1 - 2 * core
    odd = me % 2 == 1
    even = me % 2 == 0
    first_dp = dme + (1 - me % 2) * (1 - 2 * core)

    def wait_bytes(ref, sem):
        pltpu.make_async_copy(ref, ref, sem).wait()

    table = pltpu.make_async_copy(tab_ref.at[me], cs, tab_sem)
    table.start()
    firsts = [
        pltpu.make_async_copy(src, dst, first_sem.at[i])
        for i, (src, dst) in enumerate(
            ((k_hbm, k_ref), (v_hbm, v_ref), (km_hbm, km_ref), (vm_hbm, vm_ref))
        )
    ]
    for copy in firsts:
        copy.start()
    fetch_q = pltpu.make_async_copy(q_hbm, q_ref, in_sem.at[0])
    fetch_do = pltpu.make_async_copy(do_hbm, do_ref, in_sem.at[1])
    fetch_x = pltpu.make_async_copy(x_hbm, xx.at[0], in_sem.at[2])

    @pl.when(even)
    def _():
        fetch_q.start()
        fetch_do.start()

    fetch_x.start()

    def to_mate(i, src, dst, recv_sem):
        return pltpu.make_async_remote_copy(
            src_ref=src, dst_ref=dst, send_sem=swap_send.at[i], recv_sem=recv_sem,
            device_id={"dp": mate}, device_id_type=MESH,
        )

    swap_kv = to_mate(0, own, kvb.at[0], in_sem.at[3])
    swaps = [
        swap_kv,
        to_mate(1, q_hbm, q_ref, in_sem.at[0]),
        to_mate(2, do_hbm, do_ref, in_sem.at[1]),
        to_mate(3, k_ref, kx, in_sem.at[4]),
    ]
    swap_x = to_mate(4, x_hbm, xx.at[1], in_sem.at[5])
    swap_pg = to_mate(7, pgb.at[pl.ds(0, t)], pgb.at[pl.ds(t, t)], in_sem.at[6])
    backs = [to_mate(5, qg_s, qg_ref, back_recv.at[0]), to_mate(6, ig_s, ig_ref, back_recv.at[1])]
    barrier = pltpu.get_barrier_semaphore()

    xs = 4 if chips == 16 else 2
    ys = chips // xs
    row, col = chip // xs, chip % xs
    beside = [(row * xs + (col + i) % xs) * 2 for i in range(1, xs)]
    above = [((row + i) % ys * xs + col) * 2 for i in range(1, ys)]

    def greet(where):
        pl.semaphore_signal(barrier, inc=1, device_id=where, device_id_type=MESH)

    for side in (left, right):
        greet({"sp": side, "dp": dme})
        greet({"sp": side, "dp": mate})
    greet({"dp": mate})
    for other in beside + above:
        for i in range(2):
            greet({"dp": other + i})

    perm = split_pairs()
    ident = eye(t)
    ident_w = eye(KVW)
    qgain = split_gain(qgain_ref[...])
    kgain = split_gain(kgain_ref[...])
    for copy in firsts:
        copy.wait()
    kt[...] = dot(perm, k_ref[...], NT)
    w_rows = pl.ds(dme * wrow, wrow)
    w_all[w_rows, :KVW] = km_ref[...]
    w_all[w_rows, KVW:] = vm_ref[...]
    table.wait()
    cos, sin = cs[:HALF], cs[HALF:]
    rot = jnp.concatenate(
        [rope_fwd(kt[DIM * g : DIM * (g + 1)], cos, sin, kgain) for g in range(GROUPS)], axis=0
    ).astype(BF16)
    own[:t] = dot(ident, rot, NT).astype(BF16)
    own[t:] = v_ref[...]

    @pl.when(even)
    def _():
        kvb[0] = own[...]

    def to_right(s, c):
        part = pl.ds(c * crow, crow)
        return pltpu.make_async_remote_copy(
            src_ref=kvb.at[s - 1, part], dst_ref=kvb.at[s, part],
            send_sem=g_send, recv_sem=g_recv.at[0, s - 1, c],
            device_id={"sp": right, "dp": mate}, device_id_type=MESH,
        )

    def to_left(s, c):
        part = pl.ds(c * crow, crow)
        return pltpu.make_async_remote_copy(
            src_ref=kvb.at[(n + 1 - s) % n, part], dst_ref=kvb.at[n - s, part],
            send_sem=g_send, recv_sem=g_recv.at[1, s - 1, c],
            device_id={"sp": left, "dp": mate}, device_id_type=MESH,
        )

    def first_hop(c, d):
        part = pl.ds(c * crow, crow)
        return pltpu.make_async_remote_copy(
            src_ref=own.at[part], dst_ref=kvb.at[n - 1 if d else 1, part],
            send_sem=g_send, recv_sem=g_recv.at[d, 0, c],
            device_id={"sp": left if d else right, "dp": first_dp}, device_id_type=MESH,
        )

    def to_plane(k):
        return pltpu.make_async_remote_copy(
            src_ref=w_all.at[w_rows], dst_ref=w_all.at[w_rows],
            send_sem=w_send, recv_sem=w_recv,
            device_id={"dp": (dme + k) % nd}, device_id_type=MESH,
        )

    pl.semaphore_wait(barrier, 5 + 2 * len(beside + above))
    for other in beside:
        for i in range(2):
            pl.semaphore_signal(plane, inc=1, device_id={"dp": other + i}, device_id_type=MESH)
    for c in range(PARTS):
        first_hop(c, 0).start()
        first_hop(c, 1).start()

    @pl.when(odd)
    def _():
        for copy in swaps:
            copy.start()

    swap_x.start()


    def start_w(k, _):
        to_plane(k).start()
        return 0

    fetch_q.wait()
    fetch_do.wait()
    qbd[...] = jnp.zeros_like(qbd)
    obd[...] = jnp.zeros_like(obd)
    for g in range(GROUPS):
        tr = dot(perm, q_ref[:, KVW * g : KVW * (g + 1)], NT)
        qt[g] = tr
        ot = dot(ident_w, do_ref[:, KVW * g : KVW * (g + 1)], NT).astype(BF16)
        for i in range(PER):
            rows = slice(DIM * i, DIM * (i + 1))
            qr = rope_fwd(tr[rows], cos, sin, qgain).astype(BF16) * jnp.asarray(SCALE, BF16)
            cols = slice(w * g + t * i, w * g + t * (i + 1))
            qbd[DIM * g : DIM * (g + 1), cols] = qr
            obd[DIM * g : DIM * (g + 1), cols] = ot[rows]

    mrun[...] = jnp.full_like(mrun, -jnp.inf)
    lsum[...] = jnp.zeros_like(lsum)
    dsum[...] = jnp.zeros_like(dsum)
    dqt[...] = jnp.zeros_like(dqt)

    def first_pass(slots, step, g):
        cols = slice(w * g, w * (g + 1))
        kb = jnp.concatenate([kvb[r, :t] for r in slots], axis=0)
        vb = jnp.concatenate([kvb[r, t:] for r in slots], axis=0)
        s = dot(kb, qbd[:, cols])
        dp = dot(vb, obd[:, cols])
        m_old = mrun[:, cols]
        m_new = jnp.maximum(m_old, jnp.max(s, axis=0, keepdims=True))
        e = jnp.exp(s - m_new)
        a = jnp.exp(m_old - m_new)
        mrun[:, cols] = m_new
        mj[step, :, cols] = m_new
        lsum[:, cols] = lsum[:, cols] * a + jnp.sum(e, axis=0, keepdims=True)
        dsum[:, cols] = dsum[:, cols] * a + jnp.sum(e * dp, axis=0, keepdims=True)
        for i, r in enumerate(slots):
            e_ref[r, :, cols] = e[t * i : t * (i + 1)]
            dp_ref[r, :, cols] = dp[t * i : t * (i + 1)]

    pl.when(odd)(swap_kv.wait_recv)
    for g in range(GROUPS):
        first_pass((0,), 0, g)
    for i in range(GROUPS * PER):
        cols = slice(t * i, t * (i + 1))
        qbdt[cols, :] = dot(ident, qbd[:, cols], NT).astype(BF16)
        obdt[cols, :] = dot(ident, obd[:, cols], NT).astype(BF16)

    for c in range(PARTS):
        to_right(1, c).wait_recv()
        if h > 2 or c < PARTS // 2:
            to_right(2, c).start()
        to_left(1, c).wait_recv()
        if h > 2 or c >= PARTS // 2:
            to_left(2, c).start()

    def gather_step(s, _):
        @pl.when(s == min(3, h))
        def _():
            pl.semaphore_wait(plane, 2 * len(beside))
            lax.fori_loop(1, nd, start_w, 0)

        for c in range(PARTS):
            def receive(copy, s=s, c=c):
                copy(s, c).wait_recv()

            def forward(copy, s=s, c=c):
                copy(s + 1, c).start()

            for copy, whole in ((to_right, c < PARTS // 2), (to_left, c >= PARTS // 2)):
                if whole:
                    receive(copy)
                    pl.when(s < h)(functools.partial(forward, copy))
                else:
                    pl.when(s < h)(functools.partial(receive, copy))
                    pl.when(s < h - 1)(functools.partial(forward, copy))
            first_pass((s - 1, n + 1 - s), s - 1, c)
        return 0

    lax.fori_loop(2, h + 1, gather_step, 0)
    for g in range(GROUPS):
        first_pass((h,), h, g)

    lsum[...] = 1.0 / lsum[...]
    dsum[...] = dsum[...] * lsum[...]

    def second_pass(slots, step, g, place):
        cols = slice(w * g, w * (g + 1))
        half = slice(HALFW * (g // 2), HALFW * (g // 2 + 1))
        rows = len(slots) * t
        kb = jnp.concatenate([kvb[r, :t] for r in slots], axis=0)
        ktg = dot(ident_w[DIM * g : DIM * (g + 1)], kb, NT).astype(BF16)
        coef = jnp.exp(mj[step, :, cols] - mrun[:, cols]) * lsum[:, cols]
        e = jnp.concatenate([e_ref[r, :, cols] for r in slots], axis=0)
        dp = jnp.concatenate([dp_ref[r, :, cols] for r in slots], axis=0)
        p = e * coef
        ds = (p * (dp - dsum[:, cols])).astype(BF16)
        dv = dot(p.astype(BF16), obdt[cols, half])
        dk = dot(ds, qbdt[cols, half])
        c = 2 * (g // 2)
        if g % 2 == 0:
            acc[place, c, :rows] = dv
            acc[place, c + 1, :rows] = dk
        else:
            acc[place, c, :rows] += dv
            acc[place, c + 1, :rows] += dk
        dqt[DIM * g : DIM * (g + 1)] += dot(ktg, ds)

    def pass_on(d, u, c, b):
        part = pl.ds(srow * b, srow)
        return pltpu.make_async_remote_copy(
            src_ref=sbuf.at[d, u, c, part], dst_ref=rbuf.at[d, u, c, part],
            send_sem=r_send, recv_sem=r_recv.at[d, u, c, b],
            device_id={"sp": left if d else right, "dp": mate}, device_id_type=MESH,
        )

    for c in range(CHUNKS):
        rbuf[c % 2, 0, c] = jnp.zeros((t, HALFW), BF16)
    for g in range(GROUPS):
        second_pass((h,), h, g, 0)
        if g % 2 == 1:
            for c in (g - 1, g):
                d = 1 - c % 2
                sbuf[d, 0, c] = acc[0, c, :t].astype(BF16)
                for b in range(SUBS):
                    pass_on(d, 0, c, b).start()
    for g in range(GROUPS):
        second_pass((h + 1, h - 1), h - 1, g, 1)

    def add_and_send(u, c, place):
        for b in range(SUBS):
            for d in range(2):
                def arrived(d=d, b=b):
                    pass_on(d, u - 1, c, b).wait_recv()

                if d == 1 - c % 2:
                    arrived()
                else:
                    pl.when(u > 1)(arrived)
                part = slice(srow * b, srow * (b + 1))
                own = acc[place, c, t * d + srow * b : t * d + srow * (b + 1)]
                sbuf[d, u, c, part] = (own + rbuf[d, u - 1, c, part].astype(F32)).astype(BF16)
                pass_on(d, u, c, b).start()

    def reduce_step(u, _):
        for c in range(CHUNKS):
            add_and_send(u, c, u % 2)
            second_pass((h + 1 + u, h - 1 - u), h - 1 - u, c, (u + 1) % 2)
        return 0

    lax.fori_loop(1, h - 1, reduce_step, 0)
    last = (h - 1) % 2
    for c in range(CHUNKS):
        add_and_send(h - 1, c, last)
        second_pass((0,), 0, c, 1 - last)

    perm_t = split_pairs(True)
    for g in range(GROUPS):
        y = jnp.concatenate(
            [
                rope_bwd(
                    dqt[DIM * g : DIM * (g + 1), t * i : t * (i + 1)] * SCALE,
                    qt[g, DIM * i : DIM * (i + 1)], cos, sin, qgain,
                )
                for i in range(PER)
            ],
            axis=0,
        ).astype(BF16)
        y = dot(perm_t, y).astype(BF16)
        qg_s[:, KVW * g : KVW * (g + 1)] = dot(ident, y, NT).astype(BF16)
    fetch_x.wait()
    swap_x.wait_recv()

    @pl.when(odd)
    def _():
        swaps[3].wait_recv()
        kt[...] = dot(perm, kx[...], NT)

    width = xx.shape[2]
    wide = 2 * wrow
    r = lax.broadcasted_iota(jnp.int32, (wrow, wide), 0)
    c = lax.broadcasted_iota(jnp.int32, (wrow, wide), 1)
    pick = (c == r + core * wrow).astype(F32).astype(BF16)
    for part in range(2):
        j = (me + part) % 2
        for i in range(chips):
            xt[wrow * i : wrow * (i + 1), t * part : t * (part + 1)] = dot(
                pick, xx[j, :, wide * i : wide * (i + 1)], NT
            ).astype(BF16)

    whole = []
    for c in range(CHUNKS):
        for b in range(SUBS):
            for d in range(2):
                pass_on(d, h - 1, c, b).wait_recv()
        whole.append(
            acc[1 - last, c, :t] + rbuf[0, h - 1, c].astype(F32) + rbuf[1, h - 1, c].astype(F32)
        )
    dkt = jnp.transpose(jnp.concatenate([whole[1], whole[3]], axis=1))
    y = jnp.concatenate(
        [
            rope_bwd(dkt[DIM * g : DIM * (g + 1)], kt[DIM * g : DIM * (g + 1)], cos, sin, kgain)
            for g in range(GROUPS)
        ],
        axis=0,
    ).astype(BF16)
    y = dot(perm_t, y).astype(BF16)
    pgb[:t, :KVW] = dot(ident, y, NT).astype(BF16)
    pgb[:t, KVW : KVW + HALFW] = whole[0].astype(BF16)
    pgb[:t, KVW + HALFW :] = whole[2].astype(BF16)
    swap_pg.start()

    def to_chip(k):
        return pltpu.make_async_remote_copy(
            src_ref=asend.at[(chip + k) % chips], dst_ref=arecv.at[k], send_sem=a_send, recv_sem=a_recv.at[k],
            device_id={"dp": ((chip + k) % chips) * 2 + core}, device_id_type=MESH,
        )

    wait_bytes(w_all.at[pl.ds(0, wrow * (nd - 1))], w_recv)
    pg = pgb[:t]
    for i in range(width // KVW):
        rows = slice(KVW * i, KVW * (i + 1))
        ig_s[:, rows] = dot(pg, w_all[rows, :], NT).astype(BF16)
    swap_pg.wait_recv()
    per_dot = min(4, chips)
    for i in range(chips // per_dot):
        part = dot(xt[wrow * per_dot * i : wrow * per_dot * (i + 1)], pgb[...]).astype(BF16)
        for j in range(per_dot):
            asend[per_dot * i + j] = part[wrow * j : wrow * (j + 1)]

    def send_chip(k, _):
        to_chip(k).start()
        return 0

    lax.fori_loop(1, chips, send_chip, 0)

    @pl.when(even)
    def _():
        qg_ref[...] = qg_s[...]
        ig_ref[...] = ig_s[...]

    def take_chip(k, total):
        to_chip(k).wait_recv()
        return total + arecv[k].astype(F32)

    mine = lax.fori_loop(1, chips, take_chip, asend[chip].astype(F32)).astype(BF16)

    @pl.when(odd)
    def _():
        for copy in backs:
            copy.start()


    zrow = zsend.shape[1]
    ncol = 2 * KVW // HALFW
    for i in range(n):
        zsend[i] = mine[zrow * (i // ncol) : zrow * (i // ncol + 1), HALFW * (i % ncol) : HALFW * (i % ncol + 1)]

    def to_depth(k):
        return pltpu.make_async_remote_copy(
            src_ref=zsend.at[(me + k) % n], dst_ref=zrecv.at[k],
            send_sem=z_send, recv_sem=z_recv,
            device_id={"sp": (me + k) % n}, device_id_type=MESH,
        )

    def to_all(k):
        return pltpu.make_async_remote_copy(
            src_ref=zall.at[me], dst_ref=zall.at[me],
            send_sem=y_send, recv_sem=y_recv,
            device_id={"sp": (me + k) % n}, device_id_type=MESH,
        )

    def start_depth(k, _):
        to_depth(k).start()
        return 0

    def take_depth(k, total):
        return total + zrecv[k].astype(F32)

    def start_all(k, _):
        to_all(k).start()
        return 0

    lax.fori_loop(1, n, start_depth, 0)
    wait_bytes(zrecv.at[pl.ds(0, n - 1)], z_recv)
    piece = lax.fori_loop(1, n, take_depth, zsend[me].astype(F32))
    zall[me] = piece.astype(BF16)
    lax.fori_loop(1, n, start_all, 0)
    wait_bytes(zall.at[pl.ds(0, n - 1)], y_recv)
    @pl.when(odd)
    def _():
        for copy in backs:
            copy.wait_recv()
        for copy in swaps + backs:
            copy.wait_send()

    wait_bytes(kvb.at[pl.ds(0, n - 1)], g_send)
    wait_bytes(w_all.at[pl.ds(0, wrow * (nd - 1))], w_send)
    wait_bytes(sbuf.at[0], r_send)
    wait_bytes(sbuf.at[1, pl.ds(0, h - 1)], r_send)
    swap_x.wait_send()
    swap_pg.wait_send()
    wait_bytes(asend.at[pl.ds(0, chips - 1)], a_send)
    wait_bytes(zsend.at[pl.ds(0, n - 1)], z_send)
    wait_bytes(zall.at[pl.ds(0, n - 1)], y_send)


def results(ig, qg, zall, ig_out, qg_out, kw_out, vw_out, kw, vw, sem):
    copies = [pltpu.make_async_copy(ig, ig_out, sem.at[0]), pltpu.make_async_copy(qg, qg_out, sem.at[1])]
    for copy in copies:
        copy.start()
    n, zrow, _ = zall.shape
    ncol = 2 * KVW // HALFW
    for i in range(n):
        rows = slice(zrow * (i // ncol), zrow * (i // ncol + 1))
        col = i % ncol
        out = kw if col < ncol // 2 else vw
        col = col % (ncol // 2)
        out[rows, HALFW * col : HALFW * (col + 1)] = zall[i].astype(F32)
    copies += [pltpu.make_async_copy(kw, kw_out, sem.at[2]), pltpu.make_async_copy(vw, vw_out, sem.at[3])]
    for copy in copies[2:]:
        copy.start()
    for copy in copies:
        copy.wait()


def tables(n, t):
    pos = np.arange(n * t)
    row = (pos // GRID).astype(np.float32)
    col = (pos % GRID).astype(np.float32)
    m = DIM // 4
    inv = (np.float32(ROPE_BASE) ** (-np.arange(m, dtype=np.float32) / np.float32(m))).astype(np.float32)
    ang = np.concatenate([inv[:, None] * row, inv[:, None] * col], axis=0)
    cs = np.concatenate([np.cos(ang), np.sin(ang)], axis=0).astype(np.float32)
    return np.ascontiguousarray(cs.reshape(2 * HALF, n, t).transpose(1, 0, 2))


def on_device(n, nd, inputs, queries, keys, values, out_grad, query_gain, key_gain, key_matrix, value_matrix):
    t = inputs.shape[1]
    width = inputs.shape[2]
    wrow = key_matrix.shape[0]
    q_all = GROUPS * PER * t
    h = n // 2
    chips = nd // 2
    zrow = wrow * 2 * KVW // HALFW // n
    dma = pltpu.SemaphoreType.DMA
    vmem = pl.BlockSpec(memory_space=pltpu.VMEM)
    shape = jax.ShapeDtypeStruct
    anywhere = pl.BlockSpec(memory_space=pl.ANY)
    ig, qg, zall = pl.pallas_call(
        functools.partial(kernel, n, nd),
        out_shape=(
            pltpu.VMEM((t, width), BF16),
            pltpu.VMEM((t, GROUPS * PER * DIM), BF16),
            pltpu.VMEM((n, zrow, HALFW), BF16),
        ),
        in_specs=[anywhere] * 2 + [vmem] * 2 + [anywhere] * 6,
        out_specs=(vmem,) * 3,
        scratch_shapes=[
            pltpu.VMEM((t, KVW), BF16),
            pltpu.VMEM((t, KVW), BF16),
            pltpu.VMEM((wrow, KVW), BF16),
            pltpu.VMEM((wrow, KVW), BF16),
            pltpu.VMEM((2, t, width), BF16),
            pltpu.VMEM((t, GROUPS * PER * DIM), BF16),
            pltpu.VMEM((t, GROUPS * PER * DIM), BF16),
            pltpu.VMEM((t, KVW), BF16),
            pltpu.VMEM((2 * t, KVW), BF16),
            pltpu.VMEM((t, width), BF16),
            pltpu.VMEM((t, GROUPS * PER * DIM), BF16),
            pltpu.VMEM((2 * HALF, t), F32),
            pltpu.VMEM((n, 2 * t, KVW), BF16),
            pltpu.VMEM((width, 2 * KVW), BF16),
            pltpu.VMEM((KVW, q_all), BF16),
            pltpu.VMEM((q_all, KVW), BF16),
            pltpu.VMEM((KVW, q_all), BF16),
            pltpu.VMEM((q_all, KVW), BF16),
            pltpu.VMEM((n, t, q_all), F32),
            pltpu.VMEM((n, t, q_all), F32),
            pltpu.VMEM((h + 1, 1, q_all), F32),
            pltpu.VMEM((1, q_all), F32),
            pltpu.VMEM((1, q_all), F32),
            pltpu.VMEM((1, q_all), F32),
            pltpu.VMEM((GROUPS, KVW, t), F32),
            pltpu.VMEM((KVW, t), F32),
            pltpu.VMEM((chips * wrow, 2 * t), BF16),
            pltpu.VMEM((KVW, PER * t), F32),
            pltpu.VMEM((2, CHUNKS, 2 * t, HALFW), F32),
            pltpu.VMEM((2, h, CHUNKS, t, HALFW), BF16),
            pltpu.VMEM((2, h, CHUNKS, t, HALFW), BF16),
            pltpu.VMEM((2 * t, 2 * KVW), BF16),
            pltpu.VMEM((chips, wrow, 2 * KVW), BF16),
            pltpu.VMEM((chips, wrow, 2 * KVW), BF16),
            pltpu.VMEM((n, zrow, HALFW), BF16),
            pltpu.VMEM((n, zrow, HALFW), BF16),
            dma((4,)),
            dma((7,)),
            dma((8,)),
            dma((2,)),
            dma,
            dma,
            dma((2, h, PARTS)),
            dma,
            dma,
            dma,
            dma((2, h, CHUNKS, SUBS)),
            dma,
            dma((chips,)),
            dma,
            dma,
            dma,
            dma,
            pltpu.SemaphoreType.REGULAR,
        ],
        compiler_params=pltpu.CompilerParams(
            collective_id=0, has_side_effects=True, vmem_limit_bytes=61_000_000
        ),
    )(
        keys[0], values[0], query_gain.reshape(1, DIM), key_gain.reshape(1, DIM), key_matrix, value_matrix,
        inputs[0], queries[0], out_grad[0], jnp.asarray(tables(n, t)),
    )
    input_grad, query_grad, kw, vw = pl.pallas_call(
        results,
        out_shape=(
            shape((t, width), BF16),
            shape((t, GROUPS * PER * DIM), BF16),
            shape((wrow, KVW), F32),
            shape((wrow, KVW), F32),
        ),
        in_specs=[vmem] * 3,
        out_specs=(anywhere,) * 4,
        scratch_shapes=[pltpu.VMEM((wrow, KVW), F32), pltpu.VMEM((wrow, KVW), F32), dma((4,))],
        compiler_params=pltpu.CompilerParams(vmem_limit_bytes=4 * 1024 * 1024),
    )(ig, qg, zall)
    return input_grad[None], query_grad[None], kw, vw


def solution(mesh):
    row = P("dp", "sp", None)
    return jax.shard_map(
        functools.partial(on_device, mesh.shape["sp"], mesh.shape["dp"]),
        mesh=mesh,
        in_specs=(row, row, row, row, row, P(), P(), P("dp", None), P("dp", None)),
        out_specs=(row, row, P("dp", None), P("dp", None)),
        check_vma=False,
    )
```

```python
import functools

import jax
import jax.numpy as jnp
import numpy as np
from jax import lax
from jax.experimental import pallas as pl
from jax.experimental.pallas import tpu as pltpu
from jax.sharding import PartitionSpec as P

GROUPS = 4
PER = 4
DIM = 64
HALF = 32
GRID = 64
ROPE_BASE = 10000.0
EPS = 0.5
SCALE = 0.125
KVW = GROUPS * DIM
HALFW = 2 * DIM
CHUNKS = 4
PARTS = 4
SUBS = 1
F32 = jnp.float32
BF16 = jnp.bfloat16
MESH = pl.DeviceIdType.MESH

NN = (((1,), (0,)), ((), ()))
NT = (((1,), (1,)), ((), ()))


def dot(a, b, dims=NN):
    return lax.dot_general(a, b, dims, preferred_element_type=F32)


def split_source(shape, axis):
    r = lax.broadcasted_iota(jnp.int32, shape, axis)
    i = r % DIM
    return r - i + jnp.where(i < HALF, 2 * i, 2 * i - (DIM - 1))


def split_pairs(transposed=False):
    axis = 1 if transposed else 0
    c = lax.broadcasted_iota(jnp.int32, (KVW, KVW), 1 - axis)
    return (c == split_source((KVW, KVW), axis)).astype(F32).astype(BF16)


def split_gain(gain):
    c = lax.broadcasted_iota(jnp.int32, (DIM, DIM), 1)
    pick = c == split_source((DIM, DIM), 0)
    return jnp.sum(jnp.where(pick, gain, 0.0), axis=1, keepdims=True)


def eye(n):
    r = lax.broadcasted_iota(jnp.int32, (n, n), 0)
    c = lax.broadcasted_iota(jnp.int32, (n, n), 1)
    return (r == c).astype(F32).astype(BF16)


def inv_rms(a, b):
    ms = (jnp.sum(a * a, axis=0, keepdims=True) + jnp.sum(b * b, axis=0, keepdims=True)) * (1.0 / DIM)
    return lax.rsqrt(ms + EPS)


def rope_fwd(x, cos, sin, gain):
    a, b = x[:HALF], x[HALF:]
    r = inv_rms(a, b)
    a = a * r * gain[:HALF]
    b = b * r * gain[HALF:]
    return jnp.concatenate([a * cos - b * sin, a * sin + b * cos], axis=0)


def rope_bwd(g, x, cos, sin, gain):
    a, b = g[:HALF], g[HALF:]
    ua = (a * cos + b * sin) * gain[:HALF]
    ub = (b * cos - a * sin) * gain[HALF:]
    qa, qb = x[:HALF], x[HALF:]
    r = inv_rms(qa, qb)
    inner = (jnp.sum(ua * qa, axis=0, keepdims=True) + jnp.sum(ub * qb, axis=0, keepdims=True)) * (1.0 / DIM)
    f = r * r * inner
    return jnp.concatenate([r * (ua - qa * f), r * (ub - qb * f)], axis=0)


def plane_of(chips):
    xs = 4 if chips == 16 else 2
    return xs, chips // xs


def kernel(
    n, nd,
    k_hbm, v_hbm, qgain_ref, kgain_ref, km_hbm, vm_hbm, x_hbm, q_hbm, do_hbm, tab_ref,
    ig_ref, qg_ref, zall,
    k_ref, v_ref, km_ref, vm_ref, xx, q_ref, do_ref, kx, own, ig_s, qg_s,
    cs, kvb, w_all, qbd, qbdt, obd, obdt, e_ref, dp_ref, mj, mrun, lsum, dsum, qt, kt, xt, dqt, acc,
    sbuf, rbuf, x_row, x_col, pg_row, pg_col, a_sum, b_sum, a_in, b_in, zsend, zrecv,
    first_sem, in_sem, swap_send, back_recv, tab_sem, g_send, g_recv, w_send, w_recv, r_send, r_recv, x_send, x_recv, p_send, row_recv, col_recv, s_send, s_recv,
    z_send, z_recv, y_send, y_recv, plane,
):
    t = q_ref.shape[0]
    w = PER * t
    h = n // 2
    crow = 2 * t // PARTS
    srow = t // SUBS
    wrow = km_ref.shape[0]
    chips = nd // 2
    me = lax.axis_index("sp")
    dme = lax.axis_index("dp")
    core = dme % 2
    chip = dme // 2
    right = (me + 1) % n
    left = (me + n - 1) % n
    mate = dme + 1 - 2 * core
    odd = me % 2 == 1
    even = me % 2 == 0
    first_dp = dme + (1 - me % 2) * (1 - 2 * core)

    def wait_bytes(ref, sem):
        pltpu.make_async_copy(ref, ref, sem).wait()

    table = pltpu.make_async_copy(tab_ref.at[me], cs, tab_sem)
    table.start()
    firsts = [
        pltpu.make_async_copy(src, dst, first_sem.at[i])
        for i, (src, dst) in enumerate(
            ((k_hbm, k_ref), (v_hbm, v_ref), (km_hbm, km_ref), (vm_hbm, vm_ref))
        )
    ]
    for copy in firsts:
        copy.start()
    fetch_q = pltpu.make_async_copy(q_hbm, q_ref, in_sem.at[0])
    fetch_do = pltpu.make_async_copy(do_hbm, do_ref, in_sem.at[1])
    fetch_x = pltpu.make_async_copy(x_hbm, xx, in_sem.at[2])

    @pl.when(even)
    def _():
        fetch_q.start()
        fetch_do.start()
        fetch_x.start()

    def to_mate(i, src, dst, recv_sem):
        return pltpu.make_async_remote_copy(
            src_ref=src, dst_ref=dst, send_sem=swap_send.at[i], recv_sem=recv_sem,
            device_id={"dp": mate}, device_id_type=MESH,
        )

    swap_kv = to_mate(0, own, kvb.at[0], in_sem.at[3])
    swaps = [
        swap_kv,
        to_mate(1, q_hbm, q_ref, in_sem.at[0]),
        to_mate(2, do_hbm, do_ref, in_sem.at[1]),
        to_mate(3, k_ref, kx, in_sem.at[4]),
        to_mate(4, x_hbm, xx, in_sem.at[2]),
    ]
    backs = [to_mate(5, qg_s, qg_ref, back_recv.at[0]), to_mate(6, ig_s, ig_ref, back_recv.at[1])]
    barrier = pltpu.get_barrier_semaphore()

    xs, ys = plane_of(chips)
    row, col = chip // xs, chip % xs
    beside = [(row * xs + (col + i) % xs) * 2 for i in range(1, xs)]
    above = [((row + i) % ys * xs + col) * 2 for i in range(1, ys)]

    def greet(where):
        pl.semaphore_signal(barrier, inc=1, device_id=where, device_id_type=MESH)

    for side in (left, right):
        greet({"sp": side, "dp": dme})
        greet({"sp": side, "dp": mate})
    greet({"dp": mate})
    for other in beside + above:
        for i in range(2):
            greet({"dp": other + i})

    perm = split_pairs()
    ident = eye(t)
    ident_w = eye(KVW)
    qgain = split_gain(qgain_ref[...])
    kgain = split_gain(kgain_ref[...])
    for copy in firsts:
        copy.wait()
    kt[...] = dot(perm, k_ref[...], NT)
    w_rows = pl.ds(dme * wrow, wrow)
    w_all[w_rows, :KVW] = km_ref[...]
    w_all[w_rows, KVW:] = vm_ref[...]
    table.wait()
    cos, sin = cs[:HALF], cs[HALF:]
    rot = jnp.concatenate(
        [rope_fwd(kt[DIM * g : DIM * (g + 1)], cos, sin, kgain) for g in range(GROUPS)], axis=0
    ).astype(BF16)
    own[:t] = dot(ident, rot, NT).astype(BF16)
    own[t:] = v_ref[...]

    @pl.when(even)
    def _():
        kvb[0] = own[...]

    def to_right(s, c):
        part = pl.ds(c * crow, crow)
        return pltpu.make_async_remote_copy(
            src_ref=kvb.at[s - 1, part], dst_ref=kvb.at[s, part],
            send_sem=g_send, recv_sem=g_recv.at[0, s - 1, c],
            device_id={"sp": right, "dp": mate}, device_id_type=MESH,
        )

    def to_left(s, c):
        part = pl.ds(c * crow, crow)
        return pltpu.make_async_remote_copy(
            src_ref=kvb.at[(n + 1 - s) % n, part], dst_ref=kvb.at[n - s, part],
            send_sem=g_send, recv_sem=g_recv.at[1, s - 1, c],
            device_id={"sp": left, "dp": mate}, device_id_type=MESH,
        )

    def first_hop(c, d):
        part = pl.ds(c * crow, crow)
        return pltpu.make_async_remote_copy(
            src_ref=own.at[part], dst_ref=kvb.at[n - 1 if d else 1, part],
            send_sem=g_send, recv_sem=g_recv.at[d, 0, c],
            device_id={"sp": left if d else right, "dp": first_dp}, device_id_type=MESH,
        )

    def to_plane(k):
        return pltpu.make_async_remote_copy(
            src_ref=w_all.at[w_rows], dst_ref=w_all.at[w_rows],
            send_sem=w_send, recv_sem=w_recv,
            device_id={"dp": (dme + k) % nd}, device_id_type=MESH,
        )

    pl.semaphore_wait(barrier, 5 + 2 * len(beside + above))
    for other in beside:
        for i in range(2):
            pl.semaphore_signal(plane, inc=1, device_id={"dp": other + i}, device_id_type=MESH)
    for c in range(PARTS):
        first_hop(c, 0).start()
        first_hop(c, 1).start()

    @pl.when(odd)
    def _():
        for copy in swaps:
            copy.start()


    def start_w(k, _):
        to_plane(k).start()
        return 0

    fetch_q.wait()
    fetch_do.wait()
    qbd[...] = jnp.zeros_like(qbd)
    obd[...] = jnp.zeros_like(obd)
    for g in range(GROUPS):
        tr = dot(perm, q_ref[:, KVW * g : KVW * (g + 1)], NT)
        qt[g] = tr
        ot = dot(ident_w, do_ref[:, KVW * g : KVW * (g + 1)], NT).astype(BF16)
        for i in range(PER):
            rows = slice(DIM * i, DIM * (i + 1))
            qr = rope_fwd(tr[rows], cos, sin, qgain).astype(BF16) * jnp.asarray(SCALE, BF16)
            cols = slice(w * g + t * i, w * g + t * (i + 1))
            qbd[DIM * g : DIM * (g + 1), cols] = qr
            obd[DIM * g : DIM * (g + 1), cols] = ot[rows]

    mrun[...] = jnp.full_like(mrun, -jnp.inf)
    lsum[...] = jnp.zeros_like(lsum)
    dsum[...] = jnp.zeros_like(dsum)
    dqt[...] = jnp.zeros_like(dqt)

    def first_pass(slots, step, g):
        cols = slice(w * g, w * (g + 1))
        kb = jnp.concatenate([kvb[r, :t] for r in slots], axis=0)
        vb = jnp.concatenate([kvb[r, t:] for r in slots], axis=0)
        s = dot(kb, qbd[:, cols])
        dp = dot(vb, obd[:, cols])
        m_old = mrun[:, cols]
        m_new = jnp.maximum(m_old, jnp.max(s, axis=0, keepdims=True))
        e = jnp.exp(s - m_new)
        a = jnp.exp(m_old - m_new)
        mrun[:, cols] = m_new
        mj[step, :, cols] = m_new
        lsum[:, cols] = lsum[:, cols] * a + jnp.sum(e, axis=0, keepdims=True)
        dsum[:, cols] = dsum[:, cols] * a + jnp.sum(e * dp, axis=0, keepdims=True)
        for i, r in enumerate(slots):
            e_ref[r, :, cols] = e[t * i : t * (i + 1)]
            dp_ref[r, :, cols] = dp[t * i : t * (i + 1)]

    pl.when(odd)(swap_kv.wait_recv)
    for g in range(GROUPS):
        first_pass((0,), 0, g)
    for i in range(GROUPS * PER):
        cols = slice(t * i, t * (i + 1))
        qbdt[cols, :] = dot(ident, qbd[:, cols], NT).astype(BF16)
        obdt[cols, :] = dot(ident, obd[:, cols], NT).astype(BF16)

    for c in range(PARTS):
        to_right(1, c).wait_recv()
        if h > 2 or c < PARTS // 2:
            to_right(2, c).start()
        to_left(1, c).wait_recv()
        if h > 2 or c >= PARTS // 2:
            to_left(2, c).start()

    def in_row(j, e):
        return (row * xs + (col + j) % xs) * 2 + (core + e) % 2

    def in_col(j, e):
        return ((row + j) % ys * xs + col) * 2 + (core + e) % 2

    def to_dp(src, dst, send_sem, recv_sem, where):
        return pltpu.make_async_remote_copy(
            src_ref=src, dst_ref=dst, send_sem=send_sem, recv_sem=recv_sem,
            device_id={"dp": where}, device_id_type=MESH,
        )

    row_inputs = [
        to_dp(xt.at[:, (col + j) % xs, (core + e) % 2], x_row.at[2 * j + e], x_send.at[0], x_recv.at[0], in_row(j, e))
        for j in range(xs) for e in range(2) if j + e
    ]
    col_inputs = [
        to_dp(xt.at[(row + j) % ys, :, (core + e) % 2], x_col.at[2 * j + e], x_send.at[1], x_recv.at[1], in_col(j, e))
        for j in range(ys) for e in range(2) if j + e
    ]

    def gather_step(s, _):
        @pl.when(s == min(3, h))
        def _():
            fetch_x.wait()
            for i in range(chips):
                two = dot(eye(2 * wrow), xx[:, 2 * wrow * i : 2 * wrow * (i + 1)], NT).astype(BF16)
                xt[i // xs, i % xs, 0] = two[:wrow]
                xt[i // xs, i % xs, 1] = two[wrow:]
            pl.semaphore_wait(plane, 2 * len(beside))
            lax.fori_loop(1, nd, start_w, 0)
            x_row[0] = xt[:, col, core]
            x_col[0] = xt[row, :, core]
            for copy in row_inputs + col_inputs:
                copy.start()

        for c in range(PARTS):
            def receive(copy, s=s, c=c):
                copy(s, c).wait_recv()

            def forward(copy, s=s, c=c):
                copy(s + 1, c).start()

            for copy, whole in ((to_right, c < PARTS // 2), (to_left, c >= PARTS // 2)):
                if whole:
                    receive(copy)
                    pl.when(s < h)(functools.partial(forward, copy))
                else:
                    pl.when(s < h)(functools.partial(receive, copy))
                    pl.when(s < h - 1)(functools.partial(forward, copy))
            first_pass((s - 1, n + 1 - s), s - 1, c)
        return 0

    lax.fori_loop(2, h + 1, gather_step, 0)
    for g in range(GROUPS):
        first_pass((h,), h, g)

    lsum[...] = 1.0 / lsum[...]
    dsum[...] = dsum[...] * lsum[...]

    def second_pass(slots, step, g, place):
        cols = slice(w * g, w * (g + 1))
        half = slice(HALFW * (g // 2), HALFW * (g // 2 + 1))
        rows = len(slots) * t
        kb = jnp.concatenate([kvb[r, :t] for r in slots], axis=0)
        ktg = dot(ident_w[DIM * g : DIM * (g + 1)], kb, NT).astype(BF16)
        coef = jnp.exp(mj[step, :, cols] - mrun[:, cols]) * lsum[:, cols]
        e = jnp.concatenate([e_ref[r, :, cols] for r in slots], axis=0)
        dp = jnp.concatenate([dp_ref[r, :, cols] for r in slots], axis=0)
        p = e * coef
        ds = (p * (dp - dsum[:, cols])).astype(BF16)
        dv = dot(p.astype(BF16), obdt[cols, half])
        dk = dot(ds, qbdt[cols, half])
        c = 2 * (g // 2)
        if g % 2 == 0:
            acc[place, c, :rows] = dv
            acc[place, c + 1, :rows] = dk
        else:
            acc[place, c, :rows] += dv
            acc[place, c + 1, :rows] += dk
        dqt[DIM * g : DIM * (g + 1)] += dot(ktg, ds)

    def pass_on(d, u, c, b):
        part = pl.ds(srow * b, srow)
        return pltpu.make_async_remote_copy(
            src_ref=sbuf.at[d, u, c, part], dst_ref=rbuf.at[d, u, c, part],
            send_sem=r_send, recv_sem=r_recv.at[d, u, c, b],
            device_id={"sp": left if d else right, "dp": mate}, device_id_type=MESH,
        )

    for c in range(CHUNKS):
        rbuf[c % 2, 0, c] = jnp.zeros((t, HALFW), BF16)
    for g in range(GROUPS):
        second_pass((h,), h, g, 0)
        if g % 2 == 1:
            for c in (g - 1, g):
                d = 1 - c % 2
                sbuf[d, 0, c] = acc[0, c, :t].astype(BF16)
                for b in range(SUBS):
                    pass_on(d, 0, c, b).start()
    for g in range(GROUPS):
        second_pass((h + 1, h - 1), h - 1, g, 1)

    def add_and_send(u, c, place):
        for b in range(SUBS):
            for d in range(2):
                def arrived(d=d, b=b):
                    pass_on(d, u - 1, c, b).wait_recv()

                if d == 1 - c % 2:
                    arrived()
                else:
                    pl.when(u > 1)(arrived)
                part = slice(srow * b, srow * (b + 1))
                own = acc[place, c, t * d + srow * b : t * d + srow * (b + 1)]
                sbuf[d, u, c, part] = (own + rbuf[d, u - 1, c, part].astype(F32)).astype(BF16)
                pass_on(d, u, c, b).start()

    def reduce_step(u, _):
        for c in range(CHUNKS):
            add_and_send(u, c, u % 2)
            second_pass((h + 1 + u, h - 1 - u), h - 1 - u, c, (u + 1) % 2)
        return 0

    lax.fori_loop(1, h - 1, reduce_step, 0)
    last = (h - 1) % 2
    for c in range(CHUNKS):
        add_and_send(h - 1, c, last)
        second_pass((0,), 0, c, 1 - last)

    perm_t = split_pairs(True)
    for g in range(GROUPS):
        y = jnp.concatenate(
            [
                rope_bwd(
                    dqt[DIM * g : DIM * (g + 1), t * i : t * (i + 1)] * SCALE,
                    qt[g, DIM * i : DIM * (i + 1)], cos, sin, qgain,
                )
                for i in range(PER)
            ],
            axis=0,
        ).astype(BF16)
        y = dot(perm_t, y).astype(BF16)
        qg_s[:, KVW * g : KVW * (g + 1)] = dot(ident, y, NT).astype(BF16)

    @pl.when(odd)
    def _():
        swaps[3].wait_recv()
        kt[...] = dot(perm, kx[...], NT)

    def to_row(src, dst, where):
        return to_dp(pg_row.at[src], pg_row.at[dst], p_send.at[0], row_recv.at[dst], where)

    def to_col(src, dst, where):
        return to_dp(pg_col.at[src], pg_col.at[dst], p_send.at[1], col_recv.at[dst], where)

    def arrived(c):
        for b in range(SUBS):
            for d in range(2):
                pass_on(d, h - 1, c, b).wait_recv()
        return acc[1 - last, c, :t] + rbuf[0, h - 1, c].astype(F32) + rbuf[1, h - 1, c].astype(F32)

    pg_col[0, :, :HALFW] = arrived(0).astype(BF16)
    low = arrived(1)
    pg_col[0, :, HALFW:] = arrived(2).astype(BF16)
    for j in range(1, ys):
        to_col(0, 2 * j, in_col(j, 0)).start()
    to_col(0, 1, mate).start()
    dkt = jnp.transpose(jnp.concatenate([low, arrived(3)], axis=1))
    y = jnp.concatenate(
        [
            rope_bwd(dkt[DIM * g : DIM * (g + 1)], kt[DIM * g : DIM * (g + 1)], cos, sin, kgain)
            for g in range(GROUPS)
        ],
        axis=0,
    ).astype(BF16)
    y = dot(perm_t, y).astype(BF16)
    pg_row[0] = dot(ident, y, NT).astype(BF16)
    for j in range(1, xs):
        to_row(0, 2 * j, in_row(j, 0)).start()
    to_row(0, 1, mate).start()

    width = xx.shape[1]
    wait_bytes(w_all.at[pl.ds(0, wrow * (nd - 1))], w_recv)
    pg = jnp.concatenate([pg_row[0], pg_col[0]], axis=1)
    for i in range(width // KVW):
        rows = slice(KVW * i, KVW * (i + 1))
        ig_s[:, rows] = dot(pg, w_all[rows, :], NT).astype(BF16)

    @pl.when(even)
    def _():
        qg_ref[...] = qg_s[...]
        ig_ref[...] = ig_s[...]

    wait_bytes(x_row.at[pl.ds(1, 2 * xs - 1)], x_recv.at[0])
    wait_bytes(x_col.at[pl.ds(1, 2 * ys - 1)], x_recv.at[1])

    def row_term(i):
        return dot(x_row[i].reshape(ys * wrow, t), pg_row[i])

    def col_term(i):
        return dot(x_col[i].reshape(xs * wrow, t), pg_col[i])

    to_col(0, 1, mate).wait_recv()
    to_row(0, 1, mate).wait_recv()
    total_row = row_term(0) + row_term(1)
    total_col = col_term(0) + col_term(1)
    for j in range(1, max(xs, ys)):
        if j < ys:
            to_col(0, 2 * j, mate).wait_recv()
            to_col(2 * j, 2 * j + 1, mate).start()
        if j < xs:
            to_row(0, 2 * j, mate).wait_recv()
            to_row(2 * j, 2 * j + 1, mate).start()
    for j in range(1, ys):
        total_col += col_term(2 * j)
    for j in range(1, xs):
        total_row += row_term(2 * j)
    for j in range(1, ys):
        to_col(2 * j, 2 * j + 1, mate).wait_recv()
        total_col += col_term(2 * j + 1)
    for i in range(xs):
        b_sum[i] = total_col[wrow * i : wrow * (i + 1)].astype(BF16)
    for j in range(1, xs):
        to_row(2 * j, 2 * j + 1, mate).wait_recv()
        total_row += row_term(2 * j + 1)
    for i in range(ys):
        a_sum[i] = total_row[wrow * i : wrow * (i + 1)].astype(BF16)

    b_sums = [
        to_dp(b_sum.at[(col + j) % xs], b_in.at[j], s_send.at[1], s_recv.at[1], in_row(j, 0)) for j in range(1, xs)
    ]
    a_sums = [
        to_dp(a_sum.at[(row + j) % ys], a_in.at[j], s_send.at[0], s_recv.at[0], in_col(j, 0)) for j in range(1, ys)
    ]
    for copy in b_sums + a_sums:
        copy.start()

    @pl.when(odd)
    def _():
        for copy in backs:
            copy.start()

    of_keys = a_sum[row].astype(F32)
    of_values = b_sum[col].astype(F32)
    if xs > 1:
        wait_bytes(b_in.at[pl.ds(1, xs - 1)], s_recv.at[1])
    for j in range(1, xs):
        of_values += b_in[j].astype(F32)
    if ys > 1:
        wait_bytes(a_in.at[pl.ds(1, ys - 1)], s_recv.at[0])
    for j in range(1, ys):
        of_keys += a_in[j].astype(F32)
    mine = jnp.concatenate([of_keys, of_values], axis=1).astype(BF16)

    zrow = zsend.shape[1]
    ncol = 2 * KVW // HALFW
    for i in range(n):
        zsend[i] = mine[zrow * (i // ncol) : zrow * (i // ncol + 1), HALFW * (i % ncol) : HALFW * (i % ncol + 1)]

    def to_depth(k):
        return pltpu.make_async_remote_copy(
            src_ref=zsend.at[(me + k) % n], dst_ref=zrecv.at[k],
            send_sem=z_send, recv_sem=z_recv,
            device_id={"sp": (me + k) % n}, device_id_type=MESH,
        )

    def to_all(k):
        return pltpu.make_async_remote_copy(
            src_ref=zall.at[me], dst_ref=zall.at[me],
            send_sem=y_send, recv_sem=y_recv,
            device_id={"sp": (me + k) % n}, device_id_type=MESH,
        )

    def start_depth(k, _):
        to_depth(k).start()
        return 0

    def take_depth(k, total):
        return total + zrecv[k].astype(F32)

    def start_all(k, _):
        to_all(k).start()
        return 0

    lax.fori_loop(1, n, start_depth, 0)
    wait_bytes(zrecv.at[pl.ds(0, n - 1)], z_recv)
    piece = lax.fori_loop(1, n, take_depth, zsend[me].astype(F32))
    zall[me] = piece.astype(BF16)
    lax.fori_loop(1, n, start_all, 0)
    wait_bytes(zall.at[pl.ds(0, n - 1)], y_recv)
    @pl.when(odd)
    def _():
        for copy in backs:
            copy.wait_recv()
        for copy in swaps + backs:
            copy.wait_send()

    wait_bytes(kvb.at[pl.ds(0, n - 1)], g_send)
    wait_bytes(w_all.at[pl.ds(0, wrow * (nd - 1))], w_send)
    wait_bytes(sbuf.at[0], r_send)
    wait_bytes(sbuf.at[1, pl.ds(0, h - 1)], r_send)
    wait_bytes(x_row.at[pl.ds(1, 2 * xs - 1)], x_send.at[0])
    wait_bytes(x_col.at[pl.ds(1, 2 * ys - 1)], x_send.at[1])
    wait_bytes(pg_row.at[pl.ds(1, 2 * xs - 1)], p_send.at[0])
    wait_bytes(pg_col.at[pl.ds(1, 2 * ys - 1)], p_send.at[1])
    if xs > 1:
        wait_bytes(b_in.at[pl.ds(1, xs - 1)], s_send.at[1])
    if ys > 1:
        wait_bytes(a_in.at[pl.ds(1, ys - 1)], s_send.at[0])
    wait_bytes(zsend.at[pl.ds(0, n - 1)], z_send)
    wait_bytes(zall.at[pl.ds(0, n - 1)], y_send)


def results(ig, qg, zall, ig_out, qg_out, kw_out, vw_out, kw, vw, sem):
    copies = [pltpu.make_async_copy(ig, ig_out, sem.at[0]), pltpu.make_async_copy(qg, qg_out, sem.at[1])]
    for copy in copies:
        copy.start()
    n, zrow, _ = zall.shape
    ncol = 2 * KVW // HALFW
    for i in range(n):
        rows = slice(zrow * (i // ncol), zrow * (i // ncol + 1))
        col = i % ncol
        out = kw if col < ncol // 2 else vw
        col = col % (ncol // 2)
        out[rows, HALFW * col : HALFW * (col + 1)] = zall[i].astype(F32)
    copies += [pltpu.make_async_copy(kw, kw_out, sem.at[2]), pltpu.make_async_copy(vw, vw_out, sem.at[3])]
    for copy in copies[2:]:
        copy.start()
    for copy in copies:
        copy.wait()


def tables(n, t):
    pos = np.arange(n * t)
    row = (pos // GRID).astype(np.float32)
    col = (pos % GRID).astype(np.float32)
    m = DIM // 4
    inv = (np.float32(ROPE_BASE) ** (-np.arange(m, dtype=np.float32) / np.float32(m))).astype(np.float32)
    ang = np.concatenate([inv[:, None] * row, inv[:, None] * col], axis=0)
    cs = np.concatenate([np.cos(ang), np.sin(ang)], axis=0).astype(np.float32)
    return np.ascontiguousarray(cs.reshape(2 * HALF, n, t).transpose(1, 0, 2))


def on_device(n, nd, inputs, queries, keys, values, out_grad, query_gain, key_gain, key_matrix, value_matrix):
    t = inputs.shape[1]
    width = inputs.shape[2]
    wrow = key_matrix.shape[0]
    q_all = GROUPS * PER * t
    h = n // 2
    chips = nd // 2
    xs, ys = plane_of(chips)
    zrow = wrow * 2 * KVW // HALFW // n
    dma = pltpu.SemaphoreType.DMA
    vmem = pl.BlockSpec(memory_space=pltpu.VMEM)
    shape = jax.ShapeDtypeStruct
    anywhere = pl.BlockSpec(memory_space=pl.ANY)
    ig, qg, zall = pl.pallas_call(
        functools.partial(kernel, n, nd),
        out_shape=(
            pltpu.VMEM((t, width), BF16),
            pltpu.VMEM((t, GROUPS * PER * DIM), BF16),
            pltpu.VMEM((n, zrow, HALFW), BF16),
        ),
        in_specs=[anywhere] * 2 + [vmem] * 2 + [anywhere] * 6,
        out_specs=(vmem,) * 3,
        scratch_shapes=[
            pltpu.VMEM((t, KVW), BF16),
            pltpu.VMEM((t, KVW), BF16),
            pltpu.VMEM((wrow, KVW), BF16),
            pltpu.VMEM((wrow, KVW), BF16),
            pltpu.VMEM((t, width), BF16),
            pltpu.VMEM((t, GROUPS * PER * DIM), BF16),
            pltpu.VMEM((t, GROUPS * PER * DIM), BF16),
            pltpu.VMEM((t, KVW), BF16),
            pltpu.VMEM((2 * t, KVW), BF16),
            pltpu.VMEM((t, width), BF16),
            pltpu.VMEM((t, GROUPS * PER * DIM), BF16),
            pltpu.VMEM((2 * HALF, t), F32),
            pltpu.VMEM((n, 2 * t, KVW), BF16),
            pltpu.VMEM((width, 2 * KVW), BF16),
            pltpu.VMEM((KVW, q_all), BF16),
            pltpu.VMEM((q_all, KVW), BF16),
            pltpu.VMEM((KVW, q_all), BF16),
            pltpu.VMEM((q_all, KVW), BF16),
            pltpu.VMEM((n, t, q_all), F32),
            pltpu.VMEM((n, t, q_all), F32),
            pltpu.VMEM((h + 1, 1, q_all), F32),
            pltpu.VMEM((1, q_all), F32),
            pltpu.VMEM((1, q_all), F32),
            pltpu.VMEM((1, q_all), F32),
            pltpu.VMEM((GROUPS, KVW, t), F32),
            pltpu.VMEM((KVW, t), F32),
            pltpu.VMEM((ys, xs, 2, wrow, t), BF16),
            pltpu.VMEM((KVW, PER * t), F32),
            pltpu.VMEM((2, CHUNKS, 2 * t, HALFW), F32),
            pltpu.VMEM((2, h, CHUNKS, t, HALFW), BF16),
            pltpu.VMEM((2, h, CHUNKS, t, HALFW), BF16),
            pltpu.VMEM((2 * xs, ys, wrow, t), BF16),
            pltpu.VMEM((2 * ys, xs, wrow, t), BF16),
            pltpu.VMEM((2 * xs, t, KVW), BF16),
            pltpu.VMEM((2 * ys, t, KVW), BF16),
            pltpu.VMEM((ys, wrow, KVW), BF16),
            pltpu.VMEM((xs, wrow, KVW), BF16),
            pltpu.VMEM((ys, wrow, KVW), BF16),
            pltpu.VMEM((xs, wrow, KVW), BF16),
            pltpu.VMEM((n, zrow, HALFW), BF16),
            pltpu.VMEM((n, zrow, HALFW), BF16),
            dma((4,)),
            dma((5,)),
            dma((7,)),
            dma((2,)),
            dma,
            dma,
            dma((2, h, PARTS)),
            dma,
            dma,
            dma,
            dma((2, h, CHUNKS, SUBS)),
            dma((2,)),
            dma((2,)),
            dma((2,)),
            dma((2 * xs,)),
            dma((2 * ys,)),
            dma((2,)),
            dma((2,)),
            dma,
            dma,
            dma,
            dma,
            pltpu.SemaphoreType.REGULAR,
        ],
        compiler_params=pltpu.CompilerParams(
            collective_id=0, has_side_effects=True, vmem_limit_bytes=61_000_000
        ),
    )(
        keys[0], values[0], query_gain.reshape(1, DIM), key_gain.reshape(1, DIM), key_matrix, value_matrix,
        inputs[0], queries[0], out_grad[0], jnp.asarray(tables(n, t)),
    )
    input_grad, query_grad, kw, vw = pl.pallas_call(
        results,
        out_shape=(
            shape((t, width), BF16),
            shape((t, GROUPS * PER * DIM), BF16),
            shape((wrow, KVW), F32),
            shape((wrow, KVW), F32),
        ),
        in_specs=[vmem] * 3,
        out_specs=(anywhere,) * 4,
        scratch_shapes=[pltpu.VMEM((wrow, KVW), F32), pltpu.VMEM((wrow, KVW), F32), dma((4,))],
        compiler_params=pltpu.CompilerParams(vmem_limit_bytes=4 * 1024 * 1024),
    )(ig, qg, zall)
    return input_grad[None], query_grad[None], kw, vw


def solution(mesh):
    row = P("dp", "sp", None)
    return jax.shard_map(
        functools.partial(on_device, mesh.shape["sp"], mesh.shape["dp"]),
        mesh=mesh,
        in_specs=(row, row, row, row, row, P(), P(), P("dp", None), P("dp", None)),
        out_specs=(row, row, P("dp", None), P("dp", None)),
        check_vma=False,
    )
```

```python
import functools

import jax
import jax.numpy as jnp
import numpy as np
from jax import lax
from jax.experimental import pallas as pl
from jax.experimental.pallas import tpu as pltpu
from jax.sharding import PartitionSpec as P

GROUPS = 4
PER = 4
DIM = 64
HALF = 32
GRID = 64
ROPE_BASE = 10000.0
EPS = 0.5
SCALE = 0.125
KVW = GROUPS * DIM
HALFW = 2 * DIM
CHUNKS = 4
PARTS = 4
SUBS = 1
F32 = jnp.float32
BF16 = jnp.bfloat16
MESH = pl.DeviceIdType.MESH

NN = (((1,), (0,)), ((), ()))
NT = (((1,), (1,)), ((), ()))


def dot(a, b, dims=NN):
    return lax.dot_general(a, b, dims, preferred_element_type=F32)


def split_source(shape, axis):
    r = lax.broadcasted_iota(jnp.int32, shape, axis)
    i = r % DIM
    return r - i + jnp.where(i < HALF, 2 * i, 2 * i - (DIM - 1))


def split_pairs(transposed=False):
    axis = 1 if transposed else 0
    c = lax.broadcasted_iota(jnp.int32, (KVW, KVW), 1 - axis)
    return (c == split_source((KVW, KVW), axis)).astype(F32).astype(BF16)


def split_gain(gain):
    c = lax.broadcasted_iota(jnp.int32, (DIM, DIM), 1)
    pick = c == split_source((DIM, DIM), 0)
    return jnp.sum(jnp.where(pick, gain, 0.0), axis=1, keepdims=True)


def eye(n):
    r = lax.broadcasted_iota(jnp.int32, (n, n), 0)
    c = lax.broadcasted_iota(jnp.int32, (n, n), 1)
    return (r == c).astype(F32).astype(BF16)


def inv_rms(a, b):
    ms = (jnp.sum(a * a, axis=0, keepdims=True) + jnp.sum(b * b, axis=0, keepdims=True)) * (1.0 / DIM)
    return lax.rsqrt(ms + EPS)


def rope_fwd(x, cos, sin, gain):
    a, b = x[:HALF], x[HALF:]
    r = inv_rms(a, b)
    a = a * r * gain[:HALF]
    b = b * r * gain[HALF:]
    return jnp.concatenate([a * cos - b * sin, a * sin + b * cos], axis=0)


def rope_bwd(g, x, cos, sin, gain):
    a, b = g[:HALF], g[HALF:]
    ua = (a * cos + b * sin) * gain[:HALF]
    ub = (b * cos - a * sin) * gain[HALF:]
    qa, qb = x[:HALF], x[HALF:]
    r = inv_rms(qa, qb)
    inner = (jnp.sum(ua * qa, axis=0, keepdims=True) + jnp.sum(ub * qb, axis=0, keepdims=True)) * (1.0 / DIM)
    f = r * r * inner
    return jnp.concatenate([r * (ua - qa * f), r * (ub - qb * f)], axis=0)


def plane_of(chips):
    xs = 4 if chips == 16 else 2
    return xs, chips // xs


def kernel(
    n, nd,
    k_hbm, v_hbm, qgain_ref, kgain_ref, km_hbm, vm_hbm, x_hbm, q_hbm, do_hbm, tab_ref,
    ig_ref, qg_ref, zall,
    k_ref, v_ref, km_ref, vm_ref, xx, q_ref, do_ref, kx, own, ig_s, qg_s,
    cs, kvb, w_all, qbd, qbdt, obd, obdt, e_ref, dp_ref, mj, mrun, lsum, dsum, qt, kt, xt, dqt, acc,
    sbuf, rbuf, x_row, x_col, pg_row, pg_col, a_sum, b_sum, a_in, b_in, zsend, zrecv,
    first_sem, in_sem, swap_send, back_recv, tab_sem, g_send, g_recv, w_send, w_recv, r_send, r_recv, x_send, x_recv, p_send, row_recv, col_recv, s_send, s_recv,
    z_send, z_recv, y_send, y_recv, plane,
):
    t = q_ref.shape[0]
    w = PER * t
    h = n // 2
    crow = 2 * t // PARTS
    srow = t // SUBS
    wrow = km_ref.shape[0]
    chips = nd // 2
    me = lax.axis_index("sp")
    dme = lax.axis_index("dp")
    core = dme % 2
    chip = dme // 2
    right = (me + 1) % n
    left = (me + n - 1) % n
    mate = dme + 1 - 2 * core
    odd = me % 2 == 1
    even = me % 2 == 0
    first_dp = dme + (1 - me % 2) * (1 - 2 * core)

    def wait_bytes(ref, sem):
        pltpu.make_async_copy(ref, ref, sem).wait()

    table = pltpu.make_async_copy(tab_ref.at[me], cs, tab_sem)
    table.start()
    firsts = [
        pltpu.make_async_copy(src, dst, first_sem.at[i])
        for i, (src, dst) in enumerate(
            ((k_hbm, k_ref), (v_hbm, v_ref), (km_hbm, km_ref), (vm_hbm, vm_ref))
        )
    ]
    for copy in firsts:
        copy.start()
    fetch_q = pltpu.make_async_copy(q_hbm, q_ref, in_sem.at[0])
    fetch_do = pltpu.make_async_copy(do_hbm, do_ref, in_sem.at[1])
    fetch_x = pltpu.make_async_copy(x_hbm, xx, in_sem.at[2])

    @pl.when(even)
    def _():
        fetch_q.start()
        fetch_do.start()
        fetch_x.start()

    def to_mate(i, src, dst, recv_sem):
        return pltpu.make_async_remote_copy(
            src_ref=src, dst_ref=dst, send_sem=swap_send.at[i], recv_sem=recv_sem,
            device_id={"dp": mate}, device_id_type=MESH,
        )

    swap_kv = to_mate(0, own, kvb.at[0], in_sem.at[3])
    swaps = [
        swap_kv,
        to_mate(1, q_hbm, q_ref, in_sem.at[0]),
        to_mate(2, do_hbm, do_ref, in_sem.at[1]),
        to_mate(3, k_ref, kx, in_sem.at[4]),
        to_mate(4, x_hbm, xx, in_sem.at[2]),
    ]
    backs = [to_mate(5, qg_s, qg_ref, back_recv.at[0]), to_mate(6, ig_s, ig_ref, back_recv.at[1])]
    barrier = pltpu.get_barrier_semaphore()

    xs, ys = plane_of(chips)
    row, col = chip // xs, chip % xs
    beside = [(row * xs + (col + i) % xs) * 2 for i in range(1, xs)]
    above = [((row + i) % ys * xs + col) * 2 for i in range(1, ys)]

    def greet(where):
        pl.semaphore_signal(barrier, inc=1, device_id=where, device_id_type=MESH)

    for side in (left, right):
        greet({"sp": side, "dp": dme})
        greet({"sp": side, "dp": mate})
    greet({"dp": mate})
    for other in beside + above:
        for i in range(2):
            greet({"dp": other + i})

    perm = split_pairs()
    ident = eye(t)
    ident_w = eye(KVW)
    qgain = split_gain(qgain_ref[...])
    kgain = split_gain(kgain_ref[...])
    for copy in firsts:
        copy.wait()
    kt[...] = dot(perm, k_ref[...], NT)
    w_rows = pl.ds(dme * wrow, wrow)
    w_all[w_rows, :KVW] = km_ref[...]
    w_all[w_rows, KVW:] = vm_ref[...]
    table.wait()
    cos, sin = cs[:HALF], cs[HALF:]
    rot = jnp.concatenate(
        [rope_fwd(kt[DIM * g : DIM * (g + 1)], cos, sin, kgain) for g in range(GROUPS)], axis=0
    ).astype(BF16)
    own[:t] = dot(ident, rot, NT).astype(BF16)
    own[t:] = v_ref[...]

    @pl.when(even)
    def _():
        kvb[0] = own[...]

    def to_right(s, c):
        part = pl.ds(c * crow, crow)
        return pltpu.make_async_remote_copy(
            src_ref=kvb.at[s - 1, part], dst_ref=kvb.at[s, part],
            send_sem=g_send, recv_sem=g_recv.at[0, s - 1, c],
            device_id={"sp": right, "dp": mate}, device_id_type=MESH,
        )

    def to_left(s, c):
        part = pl.ds(c * crow, crow)
        return pltpu.make_async_remote_copy(
            src_ref=kvb.at[(n + 1 - s) % n, part], dst_ref=kvb.at[n - s, part],
            send_sem=g_send, recv_sem=g_recv.at[1, s - 1, c],
            device_id={"sp": left, "dp": mate}, device_id_type=MESH,
        )

    def skip(c, d):
        part = pl.ds(c * crow, crow)
        return pltpu.make_async_remote_copy(
            src_ref=kvb.at[n + 2 - h if d else h - 2, part], dst_ref=kvb.at[h, part],
            send_sem=g_send, recv_sem=g_recv.at[d, h - 1, c],
            device_id={"sp": (me + (n - 2 if d else 2)) % n, "dp": dme}, device_id_type=MESH,
        )

    def first_hop(c, d):
        part = pl.ds(c * crow, crow)
        return pltpu.make_async_remote_copy(
            src_ref=own.at[part], dst_ref=kvb.at[n - 1 if d else 1, part],
            send_sem=g_send, recv_sem=g_recv.at[d, 0, c],
            device_id={"sp": left if d else right, "dp": first_dp}, device_id_type=MESH,
        )

    def to_plane(k):
        return pltpu.make_async_remote_copy(
            src_ref=w_all.at[w_rows], dst_ref=w_all.at[w_rows],
            send_sem=w_send, recv_sem=w_recv,
            device_id={"dp": (dme + k) % nd}, device_id_type=MESH,
        )

    pl.semaphore_wait(barrier, 5 + 2 * len(beside + above))
    for other in beside:
        for i in range(2):
            pl.semaphore_signal(plane, inc=1, device_id={"dp": other + i}, device_id_type=MESH)
    for c in range(PARTS):
        first_hop(c, 0).start()
        first_hop(c, 1).start()

    @pl.when(odd)
    def _():
        for copy in swaps:
            copy.start()


    def start_w(k, _):
        to_plane(k).start()
        return 0

    fetch_q.wait()
    fetch_do.wait()
    qbd[...] = jnp.zeros_like(qbd)
    obd[...] = jnp.zeros_like(obd)
    for g in range(GROUPS):
        tr = dot(perm, q_ref[:, KVW * g : KVW * (g + 1)], NT)
        qt[g] = tr
        ot = dot(ident_w, do_ref[:, KVW * g : KVW * (g + 1)], NT).astype(BF16)
        for i in range(PER):
            rows = slice(DIM * i, DIM * (i + 1))
            qr = rope_fwd(tr[rows], cos, sin, qgain).astype(BF16) * jnp.asarray(SCALE, BF16)
            cols = slice(w * g + t * i, w * g + t * (i + 1))
            qbd[DIM * g : DIM * (g + 1), cols] = qr
            obd[DIM * g : DIM * (g + 1), cols] = ot[rows]

    mrun[...] = jnp.full_like(mrun, -jnp.inf)
    lsum[...] = jnp.zeros_like(lsum)
    dsum[...] = jnp.zeros_like(dsum)
    dqt[...] = jnp.zeros_like(dqt)

    def first_pass(slots, step, g):
        cols = slice(w * g, w * (g + 1))
        kb = jnp.concatenate([kvb[r, :t] for r in slots], axis=0)
        vb = jnp.concatenate([kvb[r, t:] for r in slots], axis=0)
        s = dot(kb, qbd[:, cols])
        dp = dot(vb, obd[:, cols])
        m_old = mrun[:, cols]
        m_new = jnp.maximum(m_old, jnp.max(s, axis=0, keepdims=True))
        e = jnp.exp(s - m_new)
        a = jnp.exp(m_old - m_new)
        mrun[:, cols] = m_new
        mj[step, :, cols] = m_new
        lsum[:, cols] = lsum[:, cols] * a + jnp.sum(e, axis=0, keepdims=True)
        dsum[:, cols] = dsum[:, cols] * a + jnp.sum(e * dp, axis=0, keepdims=True)
        for i, r in enumerate(slots):
            e_ref[r, :, cols] = e[t * i : t * (i + 1)]
            dp_ref[r, :, cols] = dp[t * i : t * (i + 1)]

    pl.when(odd)(swap_kv.wait_recv)
    for g in range(GROUPS):
        first_pass((0,), 0, g)
    for i in range(GROUPS * PER):
        cols = slice(t * i, t * (i + 1))
        qbdt[cols, :] = dot(ident, qbd[:, cols], NT).astype(BF16)
        obdt[cols, :] = dot(ident, obd[:, cols], NT).astype(BF16)

    for c in range(PARTS):
        to_right(1, c).wait_recv()
        if h > 2 or c < PARTS // 2:
            to_right(2, c).start()
        to_left(1, c).wait_recv()
        if h > 2 or c >= PARTS // 2:
            to_left(2, c).start()

    def in_row(j, e):
        return (row * xs + (col + j) % xs) * 2 + (core + e) % 2

    def in_col(j, e):
        return ((row + j) % ys * xs + col) * 2 + (core + e) % 2

    def to_dp(src, dst, send_sem, recv_sem, where):
        return pltpu.make_async_remote_copy(
            src_ref=src, dst_ref=dst, send_sem=send_sem, recv_sem=recv_sem,
            device_id={"dp": where}, device_id_type=MESH,
        )

    row_inputs = [
        to_dp(xt.at[:, (col + j) % xs, (core + e) % 2], x_row.at[2 * j + e], x_send.at[0], x_recv.at[0], in_row(j, e))
        for j in range(xs) for e in range(2) if j + e
    ]
    col_inputs = [
        to_dp(xt.at[(row + j) % ys, :, (core + e) % 2], x_col.at[2 * j + e], x_send.at[1], x_recv.at[1], in_col(j, e))
        for j in range(ys) for e in range(2) if j + e
    ]

    def gather_step(s, _):
        @pl.when(s == min(3, h))
        def _():
            fetch_x.wait()
            for i in range(chips):
                two = dot(eye(2 * wrow), xx[:, 2 * wrow * i : 2 * wrow * (i + 1)], NT).astype(BF16)
                xt[i // xs, i % xs, 0] = two[:wrow]
                xt[i // xs, i % xs, 1] = two[wrow:]
            pl.semaphore_wait(plane, 2 * len(beside))
            lax.fori_loop(1, nd, start_w, 0)
            x_row[0] = xt[:, col, core]
            x_col[0] = xt[row, :, core]
            for copy in row_inputs + col_inputs:
                copy.start()

        for c in range(PARTS):
            def receive(copy, s=s, c=c):
                copy(s, c).wait_recv()

            def forward(copy, s=s, c=c):
                copy(s + 1, c).start()

            for d, copy in enumerate((to_right, to_left)):
                if d == c // (PARTS // 2):
                    receive(copy)
                    pl.when(s == h - 2)(skip(c, d).start)
                else:
                    pl.when(s < h)(functools.partial(receive, copy))
                pl.when(s < h - 1)(functools.partial(forward, copy))
            first_pass((s - 1, n + 1 - s), s - 1, c)
        return 0

    lax.fori_loop(2, h + 1, gather_step, 0)
    for g in range(GROUPS):
        first_pass((h,), h, g)

    lsum[...] = 1.0 / lsum[...]
    dsum[...] = dsum[...] * lsum[...]

    def second_pass(slots, step, g, place):
        cols = slice(w * g, w * (g + 1))
        half = slice(HALFW * (g // 2), HALFW * (g // 2 + 1))
        rows = len(slots) * t
        kb = jnp.concatenate([kvb[r, :t] for r in slots], axis=0)
        ktg = dot(ident_w[DIM * g : DIM * (g + 1)], kb, NT).astype(BF16)
        coef = jnp.exp(mj[step, :, cols] - mrun[:, cols]) * lsum[:, cols]
        e = jnp.concatenate([e_ref[r, :, cols] for r in slots], axis=0)
        dp = jnp.concatenate([dp_ref[r, :, cols] for r in slots], axis=0)
        p = e * coef
        ds = (p * (dp - dsum[:, cols])).astype(BF16)
        dv = dot(p.astype(BF16), obdt[cols, half])
        dk = dot(ds, qbdt[cols, half])
        c = 2 * (g // 2)
        if g % 2 == 0:
            acc[place, c, :rows] = dv
            acc[place, c + 1, :rows] = dk
        else:
            acc[place, c, :rows] += dv
            acc[place, c + 1, :rows] += dk
        dqt[DIM * g : DIM * (g + 1)] += dot(ktg, ds)

    def pass_on(d, u, c, b):
        part = pl.ds(srow * b, srow)
        return pltpu.make_async_remote_copy(
            src_ref=sbuf.at[d, u, c, part], dst_ref=rbuf.at[d, u, c, part],
            send_sem=r_send, recv_sem=r_recv.at[d, u, c, b],
            device_id={"sp": left if d else right, "dp": mate}, device_id_type=MESH,
        )

    def far_on(d, c):
        return pltpu.make_async_remote_copy(
            src_ref=sbuf.at[d, 0, c], dst_ref=rbuf.at[d, 0, c],
            send_sem=r_send, recv_sem=r_recv.at[d, 0, c, 0],
            device_id={"sp": (me + (n - 2 if d else 2)) % n, "dp": dme}, device_id_type=MESH,
        )

    for g in range(GROUPS):
        second_pass((h + 1, h - 1), h - 1, g, 1)
        if g % 2 == 1:
            for c in (g - 1, g):
                for d in range(2):
                    sbuf[d, 1, c] = acc[1, c, t * d : t * (d + 1)].astype(BF16)
                    pass_on(d, 1, c, 0).start()
    for g in range(GROUPS):
        second_pass((h,), h, g, 0)
        if g % 2 == 1:
            for c in (g - 1, g):
                d = 1 - c % 2
                sbuf[d, 0, c] = acc[0, c, :t].astype(BF16)
                far_on(d, c).start()
    for g in range(GROUPS):
        second_pass((h + 2, h - 2), h - 2, g, 0)

    def add_and_send(u, c, place, far=False):
        for d in range(2):
            pass_on(d, u - 1, c, 0).wait_recv()
            total = acc[place, c, t * d : t * (d + 1)] + rbuf[d, u - 1, c].astype(F32)
            if far and d == 1 - c % 2:
                far_on(d, c).wait_recv()
                total += rbuf[d, 0, c].astype(F32)
            sbuf[d, u, c] = total.astype(BF16)
            pass_on(d, u, c, 0).start()

    def reduce_step(u, _, far=False):
        for c in range(CHUNKS):
            add_and_send(u, c, u % 2, far)
            second_pass((h + 1 + u, h - 1 - u), h - 1 - u, c, (u + 1) % 2)
        return 0

    reduce_step(2, 0, True)
    lax.fori_loop(3, h - 1, reduce_step, 0)
    last = (h - 1) % 2
    for c in range(CHUNKS):
        add_and_send(h - 1, c, last)
        second_pass((0,), 0, c, 1 - last)

    perm_t = split_pairs(True)
    for g in range(GROUPS):
        y = jnp.concatenate(
            [
                rope_bwd(
                    dqt[DIM * g : DIM * (g + 1), t * i : t * (i + 1)] * SCALE,
                    qt[g, DIM * i : DIM * (i + 1)], cos, sin, qgain,
                )
                for i in range(PER)
            ],
            axis=0,
        ).astype(BF16)
        y = dot(perm_t, y).astype(BF16)
        qg_s[:, KVW * g : KVW * (g + 1)] = dot(ident, y, NT).astype(BF16)

    @pl.when(odd)
    def _():
        swaps[3].wait_recv()
        kt[...] = dot(perm, kx[...], NT)

    def to_row(src, dst, where):
        return to_dp(pg_row.at[src], pg_row.at[dst], p_send.at[0], row_recv.at[dst], where)

    def to_col(src, dst, where):
        return to_dp(pg_col.at[src], pg_col.at[dst], p_send.at[1], col_recv.at[dst], where)

    def arrived(c):
        for b in range(SUBS):
            for d in range(2):
                pass_on(d, h - 1, c, b).wait_recv()
        return acc[1 - last, c, :t] + rbuf[0, h - 1, c].astype(F32) + rbuf[1, h - 1, c].astype(F32)

    pg_col[0, :, :HALFW] = arrived(0).astype(BF16)
    low = arrived(1)
    pg_col[0, :, HALFW:] = arrived(2).astype(BF16)
    for j in range(1, ys):
        to_col(0, 2 * j, in_col(j, 0)).start()
    to_col(0, 1, mate).start()
    dkt = jnp.transpose(jnp.concatenate([low, arrived(3)], axis=1))
    y = jnp.concatenate(
        [
            rope_bwd(dkt[DIM * g : DIM * (g + 1)], kt[DIM * g : DIM * (g + 1)], cos, sin, kgain)
            for g in range(GROUPS)
        ],
        axis=0,
    ).astype(BF16)
    y = dot(perm_t, y).astype(BF16)
    pg_row[0] = dot(ident, y, NT).astype(BF16)
    for j in range(1, xs):
        to_row(0, 2 * j, in_row(j, 0)).start()
    to_row(0, 1, mate).start()

    width = xx.shape[1]
    wait_bytes(w_all.at[pl.ds(0, wrow * (nd - 1))], w_recv)
    pg = jnp.concatenate([pg_row[0], pg_col[0]], axis=1)
    for i in range(width // KVW):
        rows = slice(KVW * i, KVW * (i + 1))
        ig_s[:, rows] = dot(pg, w_all[rows, :], NT).astype(BF16)

    @pl.when(even)
    def _():
        qg_ref[...] = qg_s[...]
        ig_ref[...] = ig_s[...]

    wait_bytes(x_row.at[pl.ds(1, 2 * xs - 1)], x_recv.at[0])
    wait_bytes(x_col.at[pl.ds(1, 2 * ys - 1)], x_recv.at[1])

    def row_term(i):
        return dot(x_row[i].reshape(ys * wrow, t), pg_row[i])

    def col_term(i):
        return dot(x_col[i].reshape(xs * wrow, t), pg_col[i])

    to_col(0, 1, mate).wait_recv()
    to_row(0, 1, mate).wait_recv()
    total_row = row_term(0) + row_term(1)
    total_col = col_term(0) + col_term(1)
    for j in range(1, max(xs, ys)):
        if j < ys:
            to_col(0, 2 * j, mate).wait_recv()
            to_col(2 * j, 2 * j + 1, mate).start()
        if j < xs:
            to_row(0, 2 * j, mate).wait_recv()
            to_row(2 * j, 2 * j + 1, mate).start()
    for j in range(1, ys):
        total_col += col_term(2 * j)
    for j in range(1, xs):
        total_row += row_term(2 * j)
    for j in range(1, ys):
        to_col(2 * j, 2 * j + 1, mate).wait_recv()
        total_col += col_term(2 * j + 1)
    for i in range(xs):
        b_sum[i] = total_col[wrow * i : wrow * (i + 1)].astype(BF16)
    for j in range(1, xs):
        to_row(2 * j, 2 * j + 1, mate).wait_recv()
        total_row += row_term(2 * j + 1)
    for i in range(ys):
        a_sum[i] = total_row[wrow * i : wrow * (i + 1)].astype(BF16)

    b_sums = [
        to_dp(b_sum.at[(col + j) % xs], b_in.at[j], s_send.at[1], s_recv.at[1], in_row(j, 0)) for j in range(1, xs)
    ]
    a_sums = [
        to_dp(a_sum.at[(row + j) % ys], a_in.at[j], s_send.at[0], s_recv.at[0], in_col(j, 0)) for j in range(1, ys)
    ]
    for copy in b_sums + a_sums:
        copy.start()

    @pl.when(odd)
    def _():
        for copy in backs:
            copy.start()

    of_keys = a_sum[row].astype(F32)
    of_values = b_sum[col].astype(F32)
    if xs > 1:
        wait_bytes(b_in.at[pl.ds(1, xs - 1)], s_recv.at[1])
    for j in range(1, xs):
        of_values += b_in[j].astype(F32)
    if ys > 1:
        wait_bytes(a_in.at[pl.ds(1, ys - 1)], s_recv.at[0])
    for j in range(1, ys):
        of_keys += a_in[j].astype(F32)
    mine = jnp.concatenate([of_keys, of_values], axis=1).astype(BF16)

    zrow = zsend.shape[1]
    ncol = 2 * KVW // HALFW
    for i in range(n):
        zsend[i] = mine[zrow * (i // ncol) : zrow * (i // ncol + 1), HALFW * (i % ncol) : HALFW * (i % ncol + 1)]

    def to_depth(k):
        return pltpu.make_async_remote_copy(
            src_ref=zsend.at[(me + k) % n], dst_ref=zrecv.at[k],
            send_sem=z_send, recv_sem=z_recv,
            device_id={"sp": (me + k) % n}, device_id_type=MESH,
        )

    def to_all(k):
        return pltpu.make_async_remote_copy(
            src_ref=zall.at[me], dst_ref=zall.at[me],
            send_sem=y_send, recv_sem=y_recv,
            device_id={"sp": (me + k) % n}, device_id_type=MESH,
        )

    def start_depth(k, _):
        to_depth(k).start()
        return 0

    def take_depth(k, total):
        return total + zrecv[k].astype(F32)

    def start_all(k, _):
        to_all(k).start()
        return 0

    lax.fori_loop(1, n, start_depth, 0)
    wait_bytes(zrecv.at[pl.ds(0, n - 1)], z_recv)
    piece = lax.fori_loop(1, n, take_depth, zsend[me].astype(F32))
    zall[me] = piece.astype(BF16)
    lax.fori_loop(1, n, start_all, 0)
    wait_bytes(zall.at[pl.ds(0, n - 1)], y_recv)
    @pl.when(odd)
    def _():
        for copy in backs:
            copy.wait_recv()
        for copy in swaps + backs:
            copy.wait_send()

    wait_bytes(kvb.at[pl.ds(0, n - 1)], g_send)
    wait_bytes(w_all.at[pl.ds(0, wrow * (nd - 1))], w_send)
    wait_bytes(sbuf.at[0], r_send)
    wait_bytes(sbuf.at[1, pl.ds(0, h - 1)], r_send)
    wait_bytes(x_row.at[pl.ds(1, 2 * xs - 1)], x_send.at[0])
    wait_bytes(x_col.at[pl.ds(1, 2 * ys - 1)], x_send.at[1])
    wait_bytes(pg_row.at[pl.ds(1, 2 * xs - 1)], p_send.at[0])
    wait_bytes(pg_col.at[pl.ds(1, 2 * ys - 1)], p_send.at[1])
    if xs > 1:
        wait_bytes(b_in.at[pl.ds(1, xs - 1)], s_send.at[1])
    if ys > 1:
        wait_bytes(a_in.at[pl.ds(1, ys - 1)], s_send.at[0])
    wait_bytes(zsend.at[pl.ds(0, n - 1)], z_send)
    wait_bytes(zall.at[pl.ds(0, n - 1)], y_send)


def results(ig, qg, zall, ig_out, qg_out, kw_out, vw_out, kw, vw, sem):
    copies = [pltpu.make_async_copy(ig, ig_out, sem.at[0]), pltpu.make_async_copy(qg, qg_out, sem.at[1])]
    for copy in copies:
        copy.start()
    n, zrow, _ = zall.shape
    ncol = 2 * KVW // HALFW
    for i in range(n):
        rows = slice(zrow * (i // ncol), zrow * (i // ncol + 1))
        col = i % ncol
        out = kw if col < ncol // 2 else vw
        col = col % (ncol // 2)
        out[rows, HALFW * col : HALFW * (col + 1)] = zall[i].astype(F32)
    copies += [pltpu.make_async_copy(kw, kw_out, sem.at[2]), pltpu.make_async_copy(vw, vw_out, sem.at[3])]
    for copy in copies[2:]:
        copy.start()
    for copy in copies:
        copy.wait()


def tables(n, t):
    pos = np.arange(n * t)
    row = (pos // GRID).astype(np.float32)
    col = (pos % GRID).astype(np.float32)
    m = DIM // 4
    inv = (np.float32(ROPE_BASE) ** (-np.arange(m, dtype=np.float32) / np.float32(m))).astype(np.float32)
    ang = np.concatenate([inv[:, None] * row, inv[:, None] * col], axis=0)
    cs = np.concatenate([np.cos(ang), np.sin(ang)], axis=0).astype(np.float32)
    return np.ascontiguousarray(cs.reshape(2 * HALF, n, t).transpose(1, 0, 2))


def on_device(n, nd, inputs, queries, keys, values, out_grad, query_gain, key_gain, key_matrix, value_matrix):
    t = inputs.shape[1]
    width = inputs.shape[2]
    wrow = key_matrix.shape[0]
    q_all = GROUPS * PER * t
    h = n // 2
    chips = nd // 2
    xs, ys = plane_of(chips)
    zrow = wrow * 2 * KVW // HALFW // n
    dma = pltpu.SemaphoreType.DMA
    vmem = pl.BlockSpec(memory_space=pltpu.VMEM)
    shape = jax.ShapeDtypeStruct
    anywhere = pl.BlockSpec(memory_space=pl.ANY)
    ig, qg, zall = pl.pallas_call(
        functools.partial(kernel, n, nd),
        out_shape=(
            pltpu.VMEM((t, width), BF16),
            pltpu.VMEM((t, GROUPS * PER * DIM), BF16),
            pltpu.VMEM((n, zrow, HALFW), BF16),
        ),
        in_specs=[anywhere] * 2 + [vmem] * 2 + [anywhere] * 6,
        out_specs=(vmem,) * 3,
        scratch_shapes=[
            pltpu.VMEM((t, KVW), BF16),
            pltpu.VMEM((t, KVW), BF16),
            pltpu.VMEM((wrow, KVW), BF16),
            pltpu.VMEM((wrow, KVW), BF16),
            pltpu.VMEM((t, width), BF16),
            pltpu.VMEM((t, GROUPS * PER * DIM), BF16),
            pltpu.VMEM((t, GROUPS * PER * DIM), BF16),
            pltpu.VMEM((t, KVW), BF16),
            pltpu.VMEM((2 * t, KVW), BF16),
            pltpu.VMEM((t, width), BF16),
            pltpu.VMEM((t, GROUPS * PER * DIM), BF16),
            pltpu.VMEM((2 * HALF, t), F32),
            pltpu.VMEM((n, 2 * t, KVW), BF16),
            pltpu.VMEM((width, 2 * KVW), BF16),
            pltpu.VMEM((KVW, q_all), BF16),
            pltpu.VMEM((q_all, KVW), BF16),
            pltpu.VMEM((KVW, q_all), BF16),
            pltpu.VMEM((q_all, KVW), BF16),
            pltpu.VMEM((n, t, q_all), F32),
            pltpu.VMEM((n, t, q_all), F32),
            pltpu.VMEM((h + 1, 1, q_all), F32),
            pltpu.VMEM((1, q_all), F32),
            pltpu.VMEM((1, q_all), F32),
            pltpu.VMEM((1, q_all), F32),
            pltpu.VMEM((GROUPS, KVW, t), F32),
            pltpu.VMEM((KVW, t), F32),
            pltpu.VMEM((ys, xs, 2, wrow, t), BF16),
            pltpu.VMEM((KVW, PER * t), F32),
            pltpu.VMEM((2, CHUNKS, 2 * t, HALFW), F32),
            pltpu.VMEM((2, h, CHUNKS, t, HALFW), BF16),
            pltpu.VMEM((2, h, CHUNKS, t, HALFW), BF16),
            pltpu.VMEM((2 * xs, ys, wrow, t), BF16),
            pltpu.VMEM((2 * ys, xs, wrow, t), BF16),
            pltpu.VMEM((2 * xs, t, KVW), BF16),
            pltpu.VMEM((2 * ys, t, KVW), BF16),
            pltpu.VMEM((ys, wrow, KVW), BF16),
            pltpu.VMEM((xs, wrow, KVW), BF16),
            pltpu.VMEM((ys, wrow, KVW), BF16),
            pltpu.VMEM((xs, wrow, KVW), BF16),
            pltpu.VMEM((n, zrow, HALFW), BF16),
            pltpu.VMEM((n, zrow, HALFW), BF16),
            dma((4,)),
            dma((5,)),
            dma((7,)),
            dma((2,)),
            dma,
            dma,
            dma((2, h, PARTS)),
            dma,
            dma,
            dma,
            dma((2, h, CHUNKS, SUBS)),
            dma((2,)),
            dma((2,)),
            dma((2,)),
            dma((2 * xs,)),
            dma((2 * ys,)),
            dma((2,)),
            dma((2,)),
            dma,
            dma,
            dma,
            dma,
            pltpu.SemaphoreType.REGULAR,
        ],
        compiler_params=pltpu.CompilerParams(
            collective_id=0, has_side_effects=True, vmem_limit_bytes=61_000_000
        ),
    )(
        keys[0], values[0], query_gain.reshape(1, DIM), key_gain.reshape(1, DIM), key_matrix, value_matrix,
        inputs[0], queries[0], out_grad[0], jnp.asarray(tables(n, t)),
    )
    input_grad, query_grad, kw, vw = pl.pallas_call(
        results,
        out_shape=(
            shape((t, width), BF16),
            shape((t, GROUPS * PER * DIM), BF16),
            shape((wrow, KVW), F32),
            shape((wrow, KVW), F32),
        ),
        in_specs=[vmem] * 3,
        out_specs=(anywhere,) * 4,
        scratch_shapes=[pltpu.VMEM((wrow, KVW), F32), pltpu.VMEM((wrow, KVW), F32), dma((4,))],
        compiler_params=pltpu.CompilerParams(vmem_limit_bytes=4 * 1024 * 1024),
    )(ig, qg, zall)
    return input_grad[None], query_grad[None], kw, vw


def solution(mesh):
    row = P("dp", "sp", None)
    return jax.shard_map(
        functools.partial(on_device, mesh.shape["sp"], mesh.shape["dp"]),
        mesh=mesh,
        in_specs=(row, row, row, row, row, P(), P(), P("dp", None), P("dp", None)),
        out_specs=(row, row, P("dp", None), P("dp", None)),
        check_vma=False,
    )
```
